256 devices in a mesh: sp: 32 (over z, x), tp: 4 (over y), dp: 2 (over core).
Axes of the slice: x: 4, y: 4, z: 8, core: 2. Of those that a mesh axis runs over, the one named last changes fastest.
Arguments:
- latent: bfloat16 [2, 6144, 2048], P('dp', 'sp'), may hold values from -6 to 6
- cond: bfloat16 [2, 2048], P('dp', 'sp'), may hold values from -6 to 6
- context: bfloat16 [2, 256, 2048], P('dp', 'sp'), may hold values from -6 to 6
- ctx_cond: bfloat16 [2048], P('sp'), may hold values from -6 to 6
- w_mod: bfloat16 [2048, 6144], P('sp', 'tp'), may hold values from -0.125 to 0.125
- norm_gain: bfloat16 [2048], replicated, may hold values from 0.099609375 to 1.8984375
- w_query: bfloat16 [2048, 1024], P(None, 'tp'), may hold values from -0.125 to 0.125
- w_key: bfloat16 [2048, 1024], P(None, 'tp'), may hold values from -0.125 to 0.125
- w_value: bfloat16 [2048, 1024], P(None, 'tp'), may hold values from -0.125 to 0.125
- w_outgate: bfloat16 [2048, 1024], P(None, 'tp'), may hold values from -0.125 to 0.125
- w_decay: bfloat16 [2048, 2, 8], P(None, None, 'tp'), may hold values from -0.125 to 0.125
- w_beta: bfloat16 [2048, 2, 8], P(None, None, 'tp'), may hold values from -0.125 to 0.125
- decay_rate: float32 [2, 8], P(None, 'tp'), may hold values from 8.138021e-06 to 0.0333333333
- decay_bias: float32 [2, 8], P(None, 'tp'), may hold values from -3 to 3
- extra_decay: float32 [2, 2, 8, 6144], P('dp', None, 'tp', 'sp'), may hold values from -0.7000977 to -1.6276042e-05
- out_gain: bfloat16 [128], replicated, may hold values from 0.099609375 to 1.8984375
- w_out: bfloat16 [1024, 2048], replicated, may hold values from -0.1875 to 0.1875
Outputs:
- mixed_out: bfloat16 [2, 6144, 2048], P('dp', ('sp', 'tp'))
The draws below stay inside these ranges and needn't reach their ends.
All inputs are finite; a program needn't handle non-finite values.
Results may differ from the reference program's by a relative error of at most 0.0067.
Values may be sent and summed in bfloat16 or wider, within the bound.
A program may use at most 128 MiB of HBM per device.

```python
import math
import jax
import jax.numpy as jnp
from jax import lax

D = 2048
HEADS = 8
HEAD = 128
BLOCK = 64
TOK_DEV = 192
SAMPLES = 2
LATENT_TOKENS = 6144
CONTEXT = 256


def draw_decay_rate(key, part):
    pick_key, fast_key, middle_key, slow_key = jax.random.split(key, 4)
    fast_share = 0.2
    middle_share = 0.3
    picked = jax.random.uniform(pick_key, (2, HEADS), jnp.float32)
    fast_rate = jnp.exp(jax.random.uniform(fast_key, (2, HEADS), jnp.float32, math.log(1.0 / 50.0), math.log(1.0 / 30.0)))
    middle_rate = jnp.exp(jax.random.uniform(middle_key, (2, HEADS), jnp.float32, math.log(0.001), math.log(0.01)))
    slow_rate = jnp.exp(jax.random.uniform(slow_key, (2, HEADS), jnp.float32, math.log(0.05 / LATENT_TOKENS), math.log(0.3 / LATENT_TOKENS)))
    return jnp.where(picked < fast_share, fast_rate, jnp.where(picked < fast_share + middle_share, middle_rate, slow_rate))


def draw_extra_decay(key, part):
    rate_key, place_key, depth_key = jax.random.split(key, 3)
    span_count = LATENT_TOKENS // TOK_DEV
    block_rates = jnp.exp(jax.random.uniform(rate_key, (SAMPLES, 2, HEADS, span_count), jnp.float32, math.log(0.1 / LATENT_TOKENS), math.log(0.6 / LATENT_TOKENS)))
    steady_state = -jnp.repeat(block_rates, TOK_DEV, axis=-1)
    third_len = LATENT_TOKENS // 3
    offsets = jax.random.randint(place_key, (SAMPLES, 2, HEADS, 3), 0, third_len)
    token_places = offsets + third_len * jnp.arange(3)
    depth_values = jnp.log(jax.random.uniform(depth_key, (SAMPLES, 2, HEADS, 3), jnp.float32, 0.5, 0.8))
    impulse_matches = (jnp.arange(LATENT_TOKENS)[None, None, None, None, :] == token_places[..., None]).astype(jnp.float32)
    return steady_state + jnp.sum(impulse_matches * depth_values[..., None], axis=-2)


def shard_levels(rng, dims, cuts, least, top_value):
    def one(axis_at, blocks):
        steps = jax.random.uniform(jax.random.fold_in(jax.random.fold_in(rng, 6), axis_at), (blocks,), jnp.float32, least / len(cuts), top_value / len(cuts))
        return jnp.repeat(jnp.exp(steps), dims[axis_at] // blocks).reshape((-1,) + (1,) * (len(dims) - axis_at - 1))

    factor_of = one(*cuts[0])
    for cut in cuts[1:]:
        factor_of = factor_of * one(*cut)
    return factor_of


def centred(rng, extent, deviation, most, cuts=(), kind=jnp.bfloat16):
    entries = deviation * jax.random.normal(rng, extent, jnp.float32)
    if cuts:
        entries = entries * shard_levels(rng, extent, cuts, -0.22, 0.18)
    return jnp.clip(entries, -most, most).astype(kind)


def setup_inputs(seed: int = 0) -> dict:
    seeds = jax.random.split(jax.random.key(seed), 18)
    return {
        "latent": centred(seeds[0], (SAMPLES, LATENT_TOKENS, D), 1.0, 6.0, ((0, 2), (1, 32))),
        "cond": centred(seeds[1], (SAMPLES, D), 1.0, 6.0, ((0, 2), (1, 32))),
        "context": centred(seeds[2], (SAMPLES, CONTEXT, D), 1.0, 6.0, ((0, 2), (1, 32))),
        "ctx_cond": centred(seeds[3], (D,), 1.0, 6.0, ((0, 32),)),
        "w_mod": centred(seeds[4], (D, 3 * D), D ** -0.5, 0.125, ((0, 32), (1, 4))),
        "norm_gain": jnp.clip(1.0 + 0.18 * jax.random.normal(seeds[5], (D,), jnp.float32), 0.099609375, 1.8984375).astype(jnp.bfloat16),
        "w_query": centred(seeds[6], (D, HEADS * HEAD), D ** -0.5, 0.125, ((1, 4),)),
        "w_key": centred(seeds[7], (D, HEADS * HEAD), D ** -0.5, 0.125, ((1, 4),)),
        "w_value": centred(seeds[8], (D, HEADS * HEAD), D ** -0.5, 0.125, ((1, 4),)),
        "w_outgate": centred(seeds[9], (D, HEADS * HEAD), D ** -0.5, 0.125, ((1, 4),)),
        "w_decay": centred(seeds[10], (D, 2, HEADS), D ** -0.5, 0.125, ((2, 4),)),
        "w_beta": centred(seeds[11], (D, 2, HEADS), D ** -0.5, 0.125, ((2, 4),)),
        "decay_rate": draw_decay_rate(jax.random.fold_in(seeds[17], 71), 0),
        "decay_bias": centred(seeds[13], (2, HEADS), 1.0, 3.0, ((1, 4),), jnp.float32),
        "extra_decay": draw_extra_decay(jax.random.fold_in(seeds[17], 71), 0),
        "out_gain": jnp.clip(1.0 + 0.18 * jax.random.normal(seeds[15], (HEAD,), jnp.float32), 0.099609375, 1.8984375).astype(jnp.bfloat16),
        "w_out": centred(seeds[16], (HEADS * HEAD, D), (HEADS * HEAD) ** -0.5, 0.1875),
    }


norm_eps = 1e-06
beta_scale = 30.0

def contract_product(einsum_form, left_op, right_op):
    return jnp.einsum(einsum_form, left_op, right_op, precision=lax.Precision.HIGHEST)

def modulate(rows_in, gain_vec, scale_row, shift_row):
    values = rows_in.astype(jnp.float32)
    normed = values * lax.rsqrt(lax.optimization_barrier(jnp.mean(values * values, axis=-1, keepdims=True)) + norm_eps)
    return (normed * gain_vec.astype(jnp.float32) * (1.0 + scale_row) + shift_row).astype(jnp.bfloat16)

def unit_normal(values):
    return values * lax.rsqrt(lax.optimization_barrier(jnp.sum(values * values, axis=-1, keepdims=True)) + norm_eps)

def head_view(raw_proj, head_count):
    return raw_proj.astype(jnp.float32).reshape(raw_proj.shape[0], head_count, -1)

def split_inputs(raw_proj, head_count, inner_width):
    row_count = raw_proj.shape[0]
    key_rows = unit_normal(jax.nn.silu(head_view(raw_proj[:, :inner_width], head_count)))
    value_rows = jax.nn.silu(head_view(raw_proj[:, inner_width:2 * inner_width], head_count))
    decay_raw = raw_proj[:, 2 * inner_width:2 * inner_width + 2 * head_count].astype(jnp.float32)
    beta_raw = raw_proj[:, 2 * inner_width + 2 * head_count:].astype(jnp.float32)
    return (key_rows, value_rows, decay_raw.reshape(row_count, 2, head_count), beta_raw.reshape(row_count, 2, head_count))

def orient(values, direction):
    if direction:
        return values[::-1]
    return values

def to_blocks(values, block_width):
    block_count = values.shape[0] // block_width
    shaped = values.reshape((block_count, block_width) + values.shape[1:])
    return jnp.moveaxis(shaped, 2, 1)

def unit_inverse(lowpart, block_width):
    positions = jnp.arange(block_width)
    result = jnp.broadcast_to(jnp.eye(block_width, dtype=jnp.float32), lowpart.shape)
    for level_index in range((block_width - 1).bit_length()):
        half_width = 1 << level_index
        same_pair = positions[:, None] // (2 * half_width) == positions[None, :] // (2 * half_width)
        lower_half = positions[:, None] // half_width % 2 == 1
        upper_half = positions[None, :] // half_width % 2 == 0
        coupling = jnp.where(same_pair & lower_half & upper_half, lowpart, 0.0)
        result = result - contract_product('nhij,nhjk->nhik', result, contract_product('nhij,nhjk->nhik', coupling, result))
    return result

def block_terms(key_rows, value_rows, log_decay, beta_rows, block_width):
    key_blocks = to_blocks(key_rows, block_width)
    value_blocks = to_blocks(value_rows, block_width)
    cumulative = jnp.cumsum(to_blocks(log_decay, block_width), axis=-1)
    beta_blocks = to_blocks(beta_rows, block_width)
    positions = jnp.arange(block_width)
    lower_mask = positions[:, None] >= positions[None, :]
    strict = positions[:, None] > positions[None, :]
    spread = cumulative[..., :, None] - cumulative[..., None, :]
    weights = jnp.where(lower_mask, jnp.exp(jnp.where(lower_mask, spread, 0.0)), 0.0)
    scaled = key_blocks * beta_blocks[..., None]
    lowpart = jnp.where(strict, contract_product('nhid,nhjd->nhij', scaled, key_blocks) * weights, 0.0)
    inverse = unit_inverse(lowpart, block_width)
    state_update = contract_product('nhij,nhjd->nhid', inverse, value_blocks * beta_blocks[..., None])
    erased_state = contract_product('nhij,nhjd->nhid', inverse, scaled * jnp.exp(cumulative)[..., None])
    final_log_decay = cumulative[..., -1]
    decayed_keys = key_blocks * jnp.exp(final_log_decay[..., None] - cumulative)[..., None]
    return ((state_update, erased_state, decayed_keys, final_log_decay), (key_blocks, cumulative, weights))

def query_terms(queries, extras):
    key_blocks, cumulative, weights = extras
    query_blocks = to_blocks(queries, key_blocks.shape[2])
    query_decayed = query_blocks * jnp.exp(cumulative)[..., None]
    query_keys = contract_product('nhid,nhjd->nhij', query_blocks, key_blocks) * weights
    return (query_decayed, query_keys)

def direction_terms(key_rows, value_rows, decay_raw, beta_raw, decay_rate, decay_bias, direction, added, block_width):
    log_decay = -decay_rate[direction] * jax.nn.softplus(decay_raw[:, direction] + decay_bias[direction]) + added
    beta_rows = jax.nn.sigmoid(beta_raw[:, direction]) * (beta_scale * decay_rate[direction])
    return block_terms(orient(key_rows, direction), orient(value_rows, direction), orient(log_decay, direction), orient(beta_rows, direction), block_width)

def carry_state(state_now, parts):

    def advance(carried_state, inputs):
        state_update, erased_state, decayed_keys, final_log_decay = inputs
        new_value_rows = state_update - contract_product('tze,tem->tzm', erased_state, carried_state)
        carried_state = carried_state * jnp.exp(final_log_decay)[:, None, None] + contract_product('rbz,rbi->rzi', decayed_keys, new_value_rows)
        return (carried_state, None)
    return lax.scan(advance, state_now, parts)[0]

def read_out(state_now, parts, query_decayed, query_keys):

    def advance(carried_state, inputs):
        state_update, erased_state, decayed_keys, final_log_decay, query_tile, query_matrix = inputs
        new_value_rows = state_update - contract_product('tze,tem->tzm', erased_state, carried_state)
        state_readout = contract_product('tze,tem->tzm', query_tile, carried_state) + contract_product('bgd,bdc->bgc', query_matrix, new_value_rows)
        carried_state = carried_state * jnp.exp(final_log_decay)[:, None, None] + contract_product('rbz,rbi->rzi', decayed_keys, new_value_rows)
        return (carried_state, state_readout)
    readouts = lax.scan(advance, state_now, parts + (query_decayed, query_keys))[1]
    block_count, head_count, block_width, value_width = readouts.shape
    return jnp.moveaxis(readouts, 1, 2).reshape(block_count * block_width, head_count, value_width)

def reference(latent, cond, context, ctx_cond, w_mod, norm_gain, w_query, w_key, w_value, w_outgate, w_decay, w_beta, decay_rate, decay_bias, extra_decay, out_gain, w_out):
    inner_width = HEADS * HEAD
    cond_all = jnp.concatenate([cond, ctx_cond[None, :]], axis=0)
    cond_rows = jax.nn.silu(cond_all.astype(jnp.float32)).astype(jnp.bfloat16)
    modulation = jnp.dot(cond_rows, w_mod, preferred_element_type=jnp.float32)
    shift_rows = modulation[:, :D]
    scale_rows = modulation[:, D:2 * D]
    gate_rows = modulation[:, 2 * D:]
    ctx_joined = jnp.concatenate([w_key, w_value, w_decay.reshape(D, 2 * HEADS), w_beta.reshape(D, 2 * HEADS)], axis=1)
    lat_joined = jnp.concatenate([w_query, w_outgate, ctx_joined], axis=1)
    zero_state = jnp.zeros((HEADS, HEAD, HEAD), jnp.float32)
    ctx_block = min(BLOCK, CONTEXT)
    results = []
    for sample in range(SAMPLES):
        ctx_in = modulate(context[sample], norm_gain, scale_rows[SAMPLES], shift_rows[SAMPLES])
        ctx_proj = jnp.dot(ctx_in, ctx_joined, preferred_element_type=jnp.float32).astype(jnp.bfloat16)
        lat_in = modulate(latent[sample], norm_gain, scale_rows[sample], shift_rows[sample])
        lat_proj = jnp.dot(lat_in, lat_joined, preferred_element_type=jnp.float32).astype(jnp.bfloat16)
        queries = unit_normal(jax.nn.silu(head_view(lat_proj[:, :inner_width], HEADS))) * HEAD ** (-0.5)
        outgate = lat_proj[:, inner_width:2 * inner_width]
        ctx_inputs = split_inputs(ctx_proj, HEADS, inner_width)
        lat_inputs = split_inputs(lat_proj[:, 2 * inner_width:], HEADS, inner_width)
        summed_out = jnp.zeros((LATENT_TOKENS, HEADS, HEAD), jnp.float32)
        for direction in range(2):
            ctx_parts = direction_terms(*ctx_inputs, decay_rate, decay_bias, direction, 0.0, ctx_block)[0]
            ctx_state = carry_state(zero_state, ctx_parts)
            lat_parts, extras = direction_terms(*lat_inputs, decay_rate, decay_bias, direction, extra_decay[sample, direction].T, BLOCK)
            query_decayed, query_keys = query_terms(orient(queries, direction), extras)
            summed_out = summed_out + orient(read_out(ctx_state, lat_parts, query_decayed, query_keys), direction)
        normed = summed_out * lax.rsqrt(lax.optimization_barrier(jnp.mean(summed_out * summed_out, axis=-1, keepdims=True)) + norm_eps)
        normed = normed * out_gain.astype(jnp.float32)
        gated = (normed * jax.nn.silu(head_view(outgate, HEADS))).reshape(LATENT_TOKENS, inner_width).astype(jnp.bfloat16)
        mixed_rows = jnp.dot(gated, w_out, preferred_element_type=jnp.float32)
        results.append((latent[sample].astype(jnp.float32) + gate_rows[sample] * mixed_rows).astype(jnp.bfloat16))
    return jnp.stack(results)
```

```python
import functools

import jax
import jax.numpy as jnp
from jax import lax
from jax.experimental import pallas as pl
from jax.experimental.pallas import tpu as pltpu
from jax.sharding import Mesh
from jax.sharding import PartitionSpec as P

D = 2048
HEAD = 128
BLOCK = 64
HEADS_DEV = 2
CHAINS = 2 * HEADS_DEV
MAP_ROWS = HEAD + 16
ZAX, XAX, YAX = "sp_0", "sp_1", "tp"
SP = (ZAX, XAX)
SP_TP = (ZAX, XAX, YAX)
MESH = pl.DeviceIdType.MESH
F32 = jnp.float32
BF16 = jnp.bfloat16

norm_eps = 1e-06
beta_scale = 30.0

NN = (((1,), (0,)), ((), ()))
NT = (((1,), (1,)), ((), ()))
TN = (((0,), (0,)), ((), ()))


def dot16(left, right, dims=NN):
    return lax.dot_general(left, right, dims, preferred_element_type=F32)


def mm1(left, right, dims=NN):
    return dot16(left.astype(BF16), right.astype(BF16), dims)


def halves(values):
    high = values.astype(BF16)
    return high, (values - high.astype(F32)).astype(BF16)


def mm3(left, right, dims=NN):
    left_high, left_low = halves(left)
    right_high, right_low = halves(right)
    return dot16(left_high, right_high, dims) + (
        dot16(left_high, right_low, dims) + dot16(left_low, right_high, dims)
    )


def mm_exact_left(left, right, dims=NN):
    high, low = halves(right)
    left = left.astype(BF16)
    return dot16(left, high, dims) + dot16(left, low, dims)


def mm_full(left, right, dims=NN):
    return lax.dot_general(
        left, right, dims, preferred_element_type=F32, precision=lax.Precision.HIGHEST
    )


def silu(values):
    return values * jax.nn.sigmoid(values)


def softplus(values):
    return jnp.maximum(values, 0.0) + jnp.log1p(jnp.exp(-jnp.abs(values)))


def unit_normal(values):
    return values * lax.rsqrt(jnp.sum(values * values, axis=-1, keepdims=True) + norm_eps)


def iota2(shape, dim):
    return lax.broadcasted_iota(jnp.int32, shape, dim)


def unit_inverses(lows, places):
    eye = (iota2((BLOCK, BLOCK), 0) == iota2((BLOCK, BLOCK), 1)).astype(F32)

    def coupling(low, place, level):
        row, col = place
        joined = (row >> (level + 1)) == (col >> (level + 1))
        mask = joined & (((row >> level) & 1) == 1) & (((col >> level) & 1) == 0)
        return jnp.where(mask, low, 0.0)

    results = [eye - coupling(low, place, 0) for low, place in zip(lows, places)]
    for level in range(1, (BLOCK - 1).bit_length()):
        inner = [
            mm3(coupling(low, place, level), result)
            for low, place, result in zip(lows, places, results)
        ]
        results = [result - mm3(result, term) for result, term in zip(results, inner)]
    return results


def chain_terms(keys, values, gram, sums, final, betas, place):
    row, col = place
    eye = iota2((BLOCK, BLOCK), 0) == iota2((BLOCK, BLOCK), 1)
    wide = jnp.broadcast_to(sums, (BLOCK, BLOCK))
    across = jnp.sum(jnp.where(eye, wide, 0.0), axis=0, keepdims=True)
    lower = row >= col
    weights = jnp.where(lower, jnp.exp(jnp.where(lower, wide - across, 0.0)), 0.0)
    low = jnp.where(row > col, gram * betas * weights, 0.0)
    grown = jnp.exp(sums)
    scaled = keys * betas
    right = jnp.concatenate([scaled * grown, values * betas], axis=1)
    decayed = keys * jnp.exp(final - sums)
    return low, right, decayed, weights, grown


def everyone(sizes):
    barrier = pltpu.get_barrier_semaphore()
    for target in sizes:
        pl.semaphore_signal(barrier, inc=1, device_id=target, device_id_type=MESH)
    pl.semaphore_wait(barrier, len(sizes))


def mod_kernel(nz, nx, ny, cond_ref, ctx_ref, w_ref, out_ref, part, slots, mine, spread, sems):
    z, x, y = lax.axis_index(ZAX), lax.axis_index(XAX), lax.axis_index(YAX)
    send1, recv1, send2, recv2 = sems
    chunk = part.shape[2]
    first = [
        (dz, dx, {ZAX: lax.rem(z + dz, nz), XAX: lax.rem(x + dx, nx)})
        for dz in range(nz)
        for dx in range(nx)
        if (dz, dx) != (0, 0)
    ]
    second = [
        (dx, dy, {XAX: lax.rem(x + dx, nx), YAX: lax.rem(y + dy, ny)})
        for dx in range(nx)
        for dy in range(ny)
        if (dx, dy) != (0, 0)
    ]
    barrier = pltpu.get_barrier_semaphore()
    peers = [t for _, _, t in first] + [t for _, dy, t in second if dy]
    for target in peers:
        pl.semaphore_signal(barrier, inc=1, device_id=target, device_id_type=MESH)
    rows = jnp.concatenate([cond_ref[...].astype(F32), ctx_ref[...].astype(F32)], axis=0)
    rows = silu(rows).astype(BF16)
    total = dot16(rows, w_ref[...])
    for j in range(nx):
        part[j] = total[:, j * chunk : (j + 1) * chunk]
    pl.semaphore_wait(barrier, len(peers))

    copies = []
    for dz, dx, target in first:
        k = dz * nx + dx
        copy = pltpu.make_async_remote_copy(
            src_ref=part.at[lax.rem(x + dx, nx)],
            dst_ref=slots.at[k],
            send_sem=send1.at[k],
            recv_sem=recv1.at[k],
            device_id=target,
            device_id_type=MESH,
        )
        copy.start()
        copies.append(copy)
    summed = part[x]
    for (dz, dx, _), copy in zip(first, copies):
        copy.wait_recv()
        summed = summed + slots[dz * nx + dx]
    mine[...] = summed
    own = y * nx + x
    late = []
    for dx, dy, target in second:
        k = dy * nx + dx
        copy = pltpu.make_async_remote_copy(
            src_ref=mine,
            dst_ref=spread.at[own],
            send_sem=send2.at[k],
            recv_sem=recv2.at[k],
            device_id=target,
            device_id_type=MESH,
        )
        copy.start()
        late.append(copy)
    spread[own] = summed
    for copy in late:
        copy.wait_recv()
    for j in range(nx * ny):
        out_ref[:, j * chunk : (j + 1) * chunk] = spread[j]
    for copy in copies + late:
        copy.wait_send()


def modulation_of(cond, ctx_cond, w_mod, nz, nx, ny):
    chunk = w_mod.shape[1] // nx
    body = functools.partial(mod_kernel, nz, nx, ny)

    def kernel(cond_ref, ctx_ref, w_ref, out_ref, part, slots, mine, spread, s1, r1, s2, r2):
        body(cond_ref, ctx_ref, w_ref, out_ref, part, slots, mine, spread, (s1, r1, s2, r2))

    return pl.pallas_call(
        kernel,
        out_shape=jax.ShapeDtypeStruct((2, w_mod.shape[1] * ny), F32),
        in_specs=[pl.BlockSpec(memory_space=pltpu.VMEM)] * 3,
        out_specs=pl.BlockSpec(memory_space=pltpu.VMEM),
        scratch_shapes=[
            pltpu.VMEM((nx, 2, chunk), F32),
            pltpu.VMEM((nz * nx, 2, chunk), F32),
            pltpu.VMEM((2, chunk), F32),
            pltpu.VMEM((nx * ny, 2, chunk), F32),
            pltpu.SemaphoreType.DMA((nz * nx,)),
            pltpu.SemaphoreType.DMA((nz * nx,)),
            pltpu.SemaphoreType.DMA((nx * ny,)),
            pltpu.SemaphoreType.DMA((nx * ny,)),
        ],
        compiler_params=pltpu.CompilerParams(collective_id=0, has_side_effects=True),
        name="modulation",
    )(cond, ctx_cond, w_mod)


def modulate(values, gain, scale, shift):
    normed = values * lax.rsqrt(jnp.mean(values * values, axis=-1, keepdims=True) + norm_eps)
    return normed * gain * (1.0 + scale) + shift


def round16(values):
    return values.astype(BF16).astype(F32)


def span_kernel(
    lat_ref, ctx_ref, mod_ref, gain_ref, wq_ref, wk_ref, wv_ref, wo_ref, wd_ref, wb_ref,
    rate_ref, bias_ref, extra_ref, maps_ref, reads_ref, base_ref, gate_ref, pack_ref, rows,
):
    span = lat_ref.shape[0]
    ctx_rows = ctx_ref.shape[0]
    blocks = span // BLOCK
    gain = gain_ref[...].astype(F32)
    rows[:span, :] = modulate(
        lat_ref[...].astype(F32), gain, mod_ref[0:1, D : 2 * D], mod_ref[0:1, :D]
    ).astype(BF16)
    ctx_in = modulate(
        ctx_ref[...].astype(F32), gain, mod_ref[1:2, D : 2 * D], mod_ref[1:2, :D]
    )
    rows[span:, :] = jnp.concatenate(
        [ctx_in, jnp.zeros((rows.shape[0] - span - ctx_rows, D), F32)], axis=0
    ).astype(BF16)
    small = jnp.concatenate(
        [ref[d].astype(F32) for ref in (wd_ref, wb_ref) for d in range(2)], axis=0
    ).astype(BF16)
    key_raw = round16(dot16(rows[...], wk_ref[...]))
    value_raw = round16(dot16(rows[...], wv_ref[...]))
    rates_raw = round16(dot16(rows[...], small, NT))
    query_raw = round16(dot16(rows[:span, :], wq_ref[...]))
    gate_ref[...] = dot16(rows[:span, :], wo_ref[...]).astype(BF16)

    ctx_rates = jnp.concatenate(
        [rates_raw[span : span + ctx_rows], jnp.zeros((ctx_rows, HEAD - 8), F32)], axis=1
    )
    for h in range(HEADS_DEV):
        lanes = slice(h * HEAD, (h + 1) * HEAD)
        pack_ref[h] = jnp.concatenate(
            [
                key_raw[span : span + ctx_rows, lanes],
                value_raw[span : span + ctx_rows, lanes],
                ctx_rates,
            ],
            axis=1,
        ).astype(BF16)

    eye_span = (iota2((span, span), 0) == iota2((span, span), 1)).astype(F32)
    added = mm_full(eye_span, extra_ref[...], NT)
    log_decay = -rate_ref[...] * softplus(rates_raw[:span, :CHAINS] + bias_ref[...]) + added
    betas = jax.nn.sigmoid(rates_raw[:span, CHAINS:]) * (beta_scale * rate_ref[...])
    row, col = iota2((BLOCK, BLOCK), 0), iota2((BLOCK, BLOCK), 1)
    places = [(row, col), (BLOCK - 1 - row, BLOCK - 1 - col)]
    tris = [(row >= col).astype(F32), (row <= col).astype(F32)]
    sums = [
        [mm_full(tris[d], log_decay[b * BLOCK : (b + 1) * BLOCK]) for b in range(blocks)]
        for d in range(2)
    ]

    jobs, lows, orders = [], [], []
    for h in range(HEADS_DEV):
        lanes = slice(h * HEAD, (h + 1) * HEAD)
        keys_h = unit_normal(silu(key_raw[:span, lanes]))
        values_h = silu(value_raw[:span, lanes])
        queries_h = unit_normal(silu(query_raw[:, lanes])) * HEAD ** (-0.5)
        for b in range(blocks):
            part = slice(b * BLOCK, (b + 1) * BLOCK)
            keys, values, queries = keys_h[part], values_h[part], queries_h[part]
            gram = mm3(keys, keys, NT)
            cross = mm1(queries, keys, NT)
            for d in range(2):
                lane = d * HEADS_DEV + h
                cums = sums[d][b][:, lane : lane + 1]
                final = cums[BLOCK - 1 : BLOCK] if d == 0 else cums[0:1]
                low, right, decayed, weights, grown = chain_terms(
                    keys, values, gram, cums, final, betas[part, lane : lane + 1], places[d]
                )
                lows.append(low)
                orders.append(places[d])
                jobs.append((h, d, b, right, decayed, cross * weights, queries * grown, final))
    inverses = unit_inverses(lows, orders)

    eye = (iota2((HEAD, HEAD), 0) == iota2((HEAD, HEAD), 1)).astype(F32)
    found = {}
    for (h, d, b, right, decayed, attend, asked, final), inverse in zip(jobs, inverses):
        solved = mm3(inverse, right)
        step = mm1(decayed, solved, TN)
        read = mm1(attend, solved)
        found[h, d, b] = (
            -step[:, :HEAD],
            step[:, HEAD:],
            asked - read[:, :HEAD],
            read[:, HEAD:],
            jnp.exp(final),
        )
    lane_of = iota2((16, 2 * HEAD), 1)
    row_of = iota2((16, 2 * HEAD), 0)
    for h in range(HEADS_DEV):
        base = [None] * blocks
        for d in range(2):
            chain = 2 * h + d
            whole = None
            for b in range(blocks) if d == 0 else reversed(range(blocks)):
                near, offset, reader, fixed, decay = found[h, d, b]
                part = slice(b * BLOCK, (b + 1) * BLOCK)
                lanes = slice(d * HEAD, (d + 1) * HEAD)
                if whole is None:
                    whole = (decay, near, offset)
                    reads_ref[h, part, lanes] = reader.astype(BF16)
                else:
                    decay_all, near_all, offset_all = whole
                    both = jnp.concatenate([near_all, offset_all], axis=1)
                    read = mm1(reader, both)
                    reads_ref[h, part, lanes] = (decay_all * reader + read[:, :HEAD]).astype(BF16)
                    fixed = fixed + read[:, HEAD:]
                    moved = mm1(near, both)
                    whole = (
                        decay * decay_all,
                        decay * near_all + decay_all * near + moved[:, :HEAD],
                        decay * offset_all + moved[:, HEAD:] + offset,
                    )
                base[b] = fixed if base[b] is None else base[b] + fixed
            put_map(maps_ref, chain, whole, lane_of, row_of)
        for b in range(blocks):
            base_ref[h, b * BLOCK : (b + 1) * BLOCK, :] = base[b]


def put_map(ref, chain, whole, lane_of, row_of):
    decay, near, offset = whole
    ref[chain, :HEAD, :] = jnp.concatenate([near, offset], axis=1).astype(BF16)
    high = round16(decay)
    middle = round16(decay - high)
    last = decay - high - middle
    pieces = jnp.where(lane_of == 0, high, jnp.where(lane_of == 1, middle, last))
    ref[chain, HEAD:, :] = jnp.where((row_of == 0) & (lane_of < 3), pieces, 0.0).astype(BF16)


def get_map(ref, index):
    pieces = ref[index, HEAD:, :].astype(F32)
    decay = jnp.sum(jnp.sum(pieces, axis=1, keepdims=True), axis=0, keepdims=True)
    return decay, ref[index, :HEAD, :]


def span_terms(latent, context, mod, gain, wq, wk, wv, wo, wd, wb, rate, bias, extra):
    span = latent.shape[0]
    ctx_rows = context.shape[0]
    inner = HEADS_DEV * HEAD
    return pl.pallas_call(
        span_kernel,
        out_shape=(
            jax.ShapeDtypeStruct((CHAINS, MAP_ROWS, 2 * HEAD), BF16),
            jax.ShapeDtypeStruct((HEADS_DEV, span, 2 * HEAD), BF16),
            jax.ShapeDtypeStruct((HEADS_DEV, span, HEAD), F32),
            jax.ShapeDtypeStruct((span, inner), BF16),
            jax.ShapeDtypeStruct((HEADS_DEV, ctx_rows, 3 * HEAD), BF16),
        ),
        in_specs=[pl.BlockSpec(memory_space=pltpu.VMEM)] * 13,
        out_specs=[pl.BlockSpec(memory_space=pltpu.VMEM)] * 5,
        scratch_shapes=[pltpu.VMEM((span + 16, D), BF16)],
        name="span_terms",
    )(latent, context, mod, gain, wq, wk, wv, wo, wd, wb, rate, bias, extra)


def context_state(ctx_all, rate, bias, direction, h):
    tokens = ctx_all.shape[0] * ctx_all.shape[1]
    data = ctx_all[...].astype(F32).reshape(tokens, 3 * HEAD)
    keys_all = unit_normal(silu(data[:, :HEAD]))
    values_all = silu(data[:, HEAD : 2 * HEAD])
    rates = data[:, 2 * HEAD :]
    lane = iota2(rates.shape, 1)
    mine = direction * HEADS_DEV + h
    decay_raw = jnp.sum(jnp.where(lane == mine, rates, 0.0), axis=1, keepdims=True)
    beta_raw = jnp.sum(jnp.where(lane == mine + CHAINS, rates, 0.0), axis=1, keepdims=True)
    log_decay = -rate * softplus(decay_raw + bias)
    betas = jax.nn.sigmoid(beta_raw) * (beta_scale * rate)
    row, col = iota2((BLOCK, BLOCK), 0), iota2((BLOCK, BLOCK), 1)
    flip = direction * (BLOCK - 1)
    sign = 1 - 2 * direction
    place = (flip + sign * row, flip + sign * col)
    tri = (place[0] >= place[1]).astype(F32)
    jobs, lows = [], []
    for b in range(tokens // BLOCK):
        part = slice(b * BLOCK, (b + 1) * BLOCK)
        sums = mm_full(tri, jnp.broadcast_to(log_decay[part], (BLOCK, HEAD)))[:, :1]
        final = jnp.sum(log_decay[part], axis=0, keepdims=True)
        keys, values = keys_all[part], values_all[part]
        gram = mm3(keys, keys, NT)
        low, right, decayed, _, _ = chain_terms(
            keys, values, gram, sums, final, betas[part], place
        )
        lows.append(low)
        jobs.append((right, decayed, final))
    steps = []
    for (right, decayed, final), inverse in zip(jobs, unit_inverses(lows, [place] * len(lows))):
        steps.append((mm1(decayed, mm3(inverse, right), TN), jnp.exp(final)))
    return steps


def chain_kernel(
    nz, nx, ny, maps_ref, pack_ref, rate_ref, bias_ref, reads_ref, base_ref, gate_ref, gain_ref,
    out_ref, slots, ctx_all, prefix, prefix_decay, sending, zslots, state, states_out, states,
    gated, gathered, ctx_steps, ctx_decay, sems,
):
    z, x, y = lax.axis_index(ZAX), lax.axis_index(XAX), lax.axis_index(YAX)
    (
        map_send, map_recv, ctx_send, ctx_recv, z_send, z_recv, st_send, st_recv, tp_send, tp_recv
    ) = sems
    h, direction = x // 2, lax.rem(x, 2)
    sign = 1 - 2 * direction
    span = base_ref.shape[1]
    part_rows = span // ny

    barrier = pltpu.get_barrier_semaphore()
    plane = [(dz, dx) for dz in range(nz) for dx in range(nx) if (dz, dx) != (0, 0)]

    def plane_target(dz, dx):
        return {ZAX: lax.rem(z + dz, nz), XAX: lax.rem(x + dx, nx)}

    for dz, dx in plane:
        pl.semaphore_signal(barrier, inc=1, device_id=plane_target(dz, dx), device_id_type=MESH)
    for dy in range(1, ny):
        pl.semaphore_signal(
            barrier, inc=1, device_id={YAX: lax.rem(y + dy, ny)}, device_id_type=MESH
        )
    slots[0] = maps_ref[x]
    me = z * nx + x
    ctx_all[me] = pack_ref[h]
    pl.semaphore_wait(barrier, len(plane) + ny - 1)

    map_copies = []
    for dx in range(1, nx):
        to = lax.rem(x + dx, nx)
        copy = pltpu.make_async_remote_copy(
            src_ref=maps_ref.at[to],
            dst_ref=slots.at[dx],
            send_sem=map_send.at[dx],
            recv_sem=map_recv.at[dx],
            device_id={XAX: to},
            device_id_type=MESH,
        )
        copy.start()
        map_copies.append(copy)
    ctx_copies = []
    for dz, dx in plane:
        target = plane_target(dz, dx)
        copy = pltpu.make_async_remote_copy(
            src_ref=pack_ref.at[target[XAX] // 2],
            dst_ref=ctx_all.at[me],
            send_sem=ctx_send.at[dz * nx + dx],
            recv_sem=ctx_recv.at[dz * nx + dx],
            device_id=target,
            device_id_type=MESH,
        )
        copy.start()
        ctx_copies.append(copy)

    for copy in map_copies:
        copy.wait_recv()
    whole = None
    for p in range(nx):
        source = p + direction * (nx - 1 - 2 * p)
        decay, both = get_map(slots, lax.rem(x - source + nx, nx))
        both_wide = both.astype(F32)
        if whole is None:
            prefix[0] = jnp.zeros((HEAD, 2 * HEAD), F32)
            prefix_decay[0] = jnp.ones((8, HEAD), F32)
            whole = (decay, both_wide)
        else:
            decay_all, all_both = whole
            prefix[p] = all_both
            prefix_decay[p] = jnp.broadcast_to(decay_all, (8, HEAD))
            moved = mm_exact_left(both[:, :HEAD], all_both)
            near = decay * all_both[:, :HEAD] + decay_all * both_wide[:, :HEAD] + moved[:, :HEAD]
            offset = decay * all_both[:, HEAD:] + both_wide[:, HEAD:] + moved[:, HEAD:]
            whole = (decay * decay_all, jnp.concatenate([near, offset], axis=1))
    decay_all, all_both = whole
    put_map(
        sending, 0, (decay_all, all_both[:, :HEAD], all_both[:, HEAD:]),
        iota2((16, 2 * HEAD), 1), iota2((16, 2 * HEAD), 0),
    )

    def z_copy(k):
        return pltpu.make_async_remote_copy(
            src_ref=sending.at[0],
            dst_ref=zslots.at[k],
            send_sem=z_send.at[k],
            recv_sem=z_recv.at[k],
            device_id={ZAX: lax.rem(z + k * sign + nz, nz)},
            device_id_type=MESH,
        )

    behind = z + direction * (nz - 1 - 2 * z)
    ahead = nz - 1 - behind
    for k in range(1, nz):

        @pl.when(k <= ahead)
        def _(k=k):
            z_copy(k).start()

    for copy in ctx_copies:
        copy.wait_recv()
    steps = context_state(ctx_all, rate_ref[direction, h], bias_ref[direction, h], direction, h)
    count = len(steps)
    for b, (step, decay) in enumerate(steps):
        ctx_steps[b] = step
        ctx_decay[b] = jnp.broadcast_to(decay, (8, HEAD))
    first = direction * (count - 1)
    state[...] = ctx_steps[first][:, HEAD:]
    for b in range(1, count):
        at = first + sign * b
        step = ctx_steps[at]
        now = state[...]
        state[...] = ctx_decay[at, 0:1, :] * now - mm3(step[:, :HEAD], now) + step[:, HEAD:]

    for k in reversed(range(1, nz)):

        @pl.when(k <= behind)
        def _(k=k):
            z_copy(k).wait_recv()
            decay, both = get_map(zslots, k)
            now = state[...]
            state[...] = (
                decay * now + mm_exact_left(both[:, :HEAD], now) + both[:, HEAD:].astype(F32)
            )

    now = state[...]
    state_copies = []

    def state_for(to):
        p = to + direction * (nx - 1 - 2 * to)
        both = prefix[p]
        return prefix_decay[p, 0:1, :] * now + mm3(both[:, :HEAD], now) + both[:, HEAD:]

    for dx in range(1, nx):
        to = lax.rem(x + dx, nx)
        states_out[dx] = state_for(to).astype(BF16)
        copy = pltpu.make_async_remote_copy(
            src_ref=states_out.at[dx],
            dst_ref=states.at[x],
            send_sem=st_send.at[dx],
            recv_sem=st_recv.at[dx],
            device_id={XAX: to},
            device_id_type=MESH,
        )
        copy.start()
        state_copies.append(copy)
    states[x] = state_for(x).astype(BF16)
    for copy in state_copies:
        copy.wait_recv()

    gain = gain_ref[...].astype(F32)
    for i in range(HEADS_DEV):
        both = jnp.concatenate([states[2 * i], states[2 * i + 1]], axis=0)
        total = dot16(reads_ref[i], both) + base_ref[i]
        normed = total * lax.rsqrt(jnp.mean(total * total, axis=-1, keepdims=True) + norm_eps)
        lanes = slice(i * HEAD, (i + 1) * HEAD)
        result = (normed * gain * silu(gate_ref[:, lanes].astype(F32))).astype(BF16)
        for t in range(ny):
            gated[t, :, lanes] = result[t * part_rows : (t + 1) * part_rows]
    tp_copies = []
    for dy in range(1, ny):
        to = lax.rem(y + dy, ny)
        copy = pltpu.make_async_remote_copy(
            src_ref=gated.at[to],
            dst_ref=gathered.at[y],
            send_sem=tp_send.at[dy],
            recv_sem=tp_recv.at[dy],
            device_id={YAX: to},
            device_id_type=MESH,
        )
        copy.start()
        tp_copies.append(copy)
    gathered[y] = gated[y]
    for copy in tp_copies:
        copy.wait_recv()
    inner = HEADS_DEV * HEAD
    for t in range(ny):
        out_ref[:, t * inner : (t + 1) * inner] = gathered[t]
    for k in range(1, nz):

        @pl.when(k <= ahead)
        def _(k=k):
            z_copy(k).wait_send()

    for copy in map_copies + ctx_copies + state_copies + tp_copies:
        copy.wait_send()


def chains(maps, pack, rate, bias, reads, base, gate, gain, nz, nx, ny):
    span = base.shape[1]
    inner = HEADS_DEV * HEAD
    ctx_rows = pack.shape[1]
    ctx_blocks = nz * nx * ctx_rows // BLOCK

    def kernel(*refs):
        chain_kernel(nz, nx, ny, *refs[:-10], refs[-10:])

    vmem = pl.BlockSpec(memory_space=pltpu.VMEM)
    smem = pl.BlockSpec(memory_space=pltpu.SMEM)
    return pl.pallas_call(
        kernel,
        out_shape=jax.ShapeDtypeStruct((span // ny, inner * ny), BF16),
        in_specs=[vmem, vmem, smem, smem, vmem, vmem, vmem, vmem],
        out_specs=vmem,
        scratch_shapes=[
            pltpu.VMEM((nx, MAP_ROWS, 2 * HEAD), BF16),
            pltpu.VMEM((nz * nx, ctx_rows, 3 * HEAD), BF16),
            pltpu.VMEM((nx, HEAD, 2 * HEAD), F32),
            pltpu.VMEM((nx, 8, HEAD), F32),
            pltpu.VMEM((1, MAP_ROWS, 2 * HEAD), BF16),
            pltpu.VMEM((nz, MAP_ROWS, 2 * HEAD), BF16),
            pltpu.VMEM((HEAD, HEAD), F32),
            pltpu.VMEM((nx, HEAD, HEAD), BF16),
            pltpu.VMEM((nx, HEAD, HEAD), BF16),
            pltpu.VMEM((ny, span // ny, inner), BF16),
            pltpu.VMEM((ny, span // ny, inner), BF16),
            pltpu.VMEM((ctx_blocks, HEAD, 2 * HEAD), F32),
            pltpu.VMEM((ctx_blocks, 8, HEAD), F32),
            pltpu.SemaphoreType.DMA((nx,)),
            pltpu.SemaphoreType.DMA((nx,)),
            pltpu.SemaphoreType.DMA((nz * nx,)),
            pltpu.SemaphoreType.DMA((nz * nx,)),
            pltpu.SemaphoreType.DMA((nz,)),
            pltpu.SemaphoreType.DMA((nz,)),
            pltpu.SemaphoreType.DMA((nx,)),
            pltpu.SemaphoreType.DMA((nx,)),
            pltpu.SemaphoreType.DMA((ny,)),
            pltpu.SemaphoreType.DMA((ny,)),
        ],
        compiler_params=pltpu.CompilerParams(collective_id=1, has_side_effects=True),
        name="chains",
    )(maps, pack, rate, bias, reads, base, gate, gain)


def out_kernel(rows_ref, w_ref, own_ref, gate_ref, out_ref):
    mixed = dot16(rows_ref[...], w_ref[...])
    out_ref[...] = (own_ref[...].astype(F32) + gate_ref[...] * mixed).astype(BF16)


def output_rows(by_rows, w_out, own_rows, gate_row):
    count, width = own_rows.shape
    tile = 512
    return pl.pallas_call(
        out_kernel,
        grid=(width // tile,),
        out_shape=jax.ShapeDtypeStruct((count, width), BF16),
        in_specs=[
            pl.BlockSpec((count, by_rows.shape[1]), lambda i: (0, 0)),
            pl.BlockSpec((w_out.shape[0], tile), lambda i: (0, i)),
            pl.BlockSpec((count, tile), lambda i: (0, i)),
            pl.BlockSpec((1, tile), lambda i: (0, i)),
        ],
        out_specs=pl.BlockSpec((count, tile), lambda i: (0, i)),
        name="output_rows",
    )(by_rows, w_out, own_rows, gate_row)


def on_device(
    latent,
    cond,
    context,
    ctx_cond,
    w_mod,
    norm_gain,
    w_query,
    w_key,
    w_value,
    w_outgate,
    w_decay,
    w_beta,
    decay_rate,
    decay_bias,
    extra_decay,
    out_gain,
    w_out,
):
    nz, nx, ny = lax.axis_size(ZAX), lax.axis_size(XAX), lax.axis_size(YAX)
    span = latent.shape[1]
    rows_out = span // ny
    mod = modulation_of(cond, ctx_cond[None, :], w_mod, nz, nx, ny)
    maps, reads, base, gate, pack = span_terms(
        latent[0],
        context[0],
        mod,
        norm_gain[None, :],
        w_query,
        w_key,
        w_value,
        w_outgate,
        jnp.transpose(w_decay, (1, 2, 0)),
        jnp.transpose(w_beta, (1, 2, 0)),
        decay_rate.reshape(1, CHAINS),
        decay_bias.reshape(1, CHAINS),
        extra_decay.reshape(CHAINS, span),
    )
    by_rows = chains(
        maps, pack, decay_rate, decay_bias, reads, base, gate, out_gain[None, :], nz, nx, ny
    )
    own_rows = lax.dynamic_slice_in_dim(latent[0], lax.axis_index(YAX) * rows_out, rows_out, 0)
    return output_rows(by_rows, w_out, own_rows, mod[0:1, 2 * D :])[None]


def solution(mesh):
    torus = Mesh(
        mesh.devices.reshape(-1, 4, mesh.shape["tp"], mesh.shape["dp"]), (ZAX, XAX, YAX, "dp")
    )
    return jax.shard_map(
        on_device,
        mesh=torus,
        in_specs=(
            P("dp", SP, None),
            P("dp", SP),
            P("dp", SP, None),
            P(SP),
            P(SP, "tp"),
            P(),
            P(None, "tp"),
            P(None, "tp"),
            P(None, "tp"),
            P(None, "tp"),
            P(None, None, "tp"),
            P(None, None, "tp"),
            P(None, "tp"),
            P(None, "tp"),
            P("dp", None, "tp", SP),
            P(),
            P(),
        ),
        out_specs=P("dp", SP_TP, None),
        check_vma=False,
    )
```

```python
import functools

import jax
import jax.numpy as jnp
from jax import lax
from jax.experimental import pallas as pl
from jax.experimental.pallas import tpu as pltpu
from jax.sharding import Mesh
from jax.sharding import PartitionSpec as P

D = 2048
HEAD = 128
BLOCK = 64
HEADS_DEV = 2
CHAINS = 2 * HEADS_DEV
HALF = HEAD // 2
MAP_ROWS = HEAD + HALF + 16
ZAX, XAX, YAX = "sp_0", "sp_1", "tp"
SP = (ZAX, XAX)
SP_TP = (ZAX, XAX, YAX)
MESH = pl.DeviceIdType.MESH
F32 = jnp.float32
BF16 = jnp.bfloat16

norm_eps = 1e-06
beta_scale = 30.0

NN = (((1,), (0,)), ((), ()))
NT = (((1,), (1,)), ((), ()))
TN = (((0,), (0,)), ((), ()))


def dot16(left, right, dims=NN):
    return lax.dot_general(left, right, dims, preferred_element_type=F32)


def mm1(left, right, dims=NN):
    return dot16(left.astype(BF16), right.astype(BF16), dims)


def halves(values):
    high = values.astype(BF16)
    return high, (values - high.astype(F32)).astype(BF16)


def mm3(left, right, dims=NN):
    left_high, left_low = halves(left)
    right_high, right_low = halves(right)
    return dot16(left_high, right_high, dims) + (
        dot16(left_high, right_low, dims) + dot16(left_low, right_high, dims)
    )


def mm_exact_left(left, right, dims=NN):
    high, low = halves(right)
    left = left.astype(BF16)
    return dot16(left, high, dims) + dot16(left, low, dims)


def mm_full(left, right, dims=NN):
    return lax.dot_general(
        left, right, dims, preferred_element_type=F32, precision=lax.Precision.HIGHEST
    )


def silu(values):
    return values * jax.nn.sigmoid(values)


def softplus(values):
    return jnp.maximum(values, 0.0) + jnp.log1p(jnp.exp(-jnp.abs(values)))


def unit_normal(values):
    return values * lax.rsqrt(jnp.sum(values * values, axis=-1, keepdims=True) + norm_eps)


def iota2(shape, dim):
    return lax.broadcasted_iota(jnp.int32, shape, dim)


def unit_inverses(lows, places):
    eye = (iota2((BLOCK, BLOCK), 0) == iota2((BLOCK, BLOCK), 1)).astype(F32)

    def coupling(low, place, level):
        row, col = place
        joined = (row >> (level + 1)) == (col >> (level + 1))
        mask = joined & (((row >> level) & 1) == 1) & (((col >> level) & 1) == 0)
        return jnp.where(mask, low, 0.0)

    results = [eye - coupling(low, place, 0) for low, place in zip(lows, places)]
    for level in range(1, (BLOCK - 1).bit_length()):
        inner = [
            mm3(coupling(low, place, level), result)
            for low, place, result in zip(lows, places, results)
        ]
        results = [result - mm3(result, term) for result, term in zip(results, inner)]
    return results


def chain_terms(keys, values, gram, sums, final, betas, place):
    row, col = place
    eye = iota2((BLOCK, BLOCK), 0) == iota2((BLOCK, BLOCK), 1)
    wide = jnp.broadcast_to(sums, (BLOCK, BLOCK))
    across = jnp.sum(jnp.where(eye, wide, 0.0), axis=0, keepdims=True)
    lower = row >= col
    weights = jnp.where(lower, jnp.exp(jnp.where(lower, wide - across, 0.0)), 0.0)
    low = jnp.where(row > col, gram * betas * weights, 0.0)
    grown = jnp.exp(sums)
    scaled = keys * betas
    right = jnp.concatenate([scaled * grown, values * betas], axis=1)
    decayed = keys * jnp.exp(final - sums)
    return low, right, decayed, weights, grown


def round16(values):
    return values.astype(BF16).astype(F32)


def pack_halves(values):
    return jnp.concatenate([values[: HEAD // 2], values[HEAD // 2 :]], axis=1)


def unpack_halves(values):
    return jnp.concatenate([values[:, : HEAD // 2], values[:, HEAD // 2 :]], axis=0)


def decay_rows(decay):
    high = round16(decay)
    middle = round16(decay - high)
    last = decay - high - middle
    row = iota2((16, HEAD), 0)
    pieces = jnp.where(row == 0, high, jnp.where(row == 1, middle, last))
    return jnp.where(row < 3, pieces, 0.0).astype(BF16)


def put_map(ref, index, decay, near, offset):
    ref[index, :HEAD, :] = near.astype(BF16)
    ref[index, HEAD : HEAD + HALF, :] = pack_halves(offset).astype(BF16)
    ref[index, HEAD + HALF :, :] = decay_rows(decay)


def get_map(ref, index):
    pieces = ref[index, HEAD + HALF :, :].astype(F32)
    decay = pieces[0:1] + pieces[1:2] + pieces[2:3]
    offset = unpack_halves(ref[index, HEAD : HEAD + HALF, :].astype(F32))
    return decay, ref[index, :HEAD, :], offset


def context_steps(ctx_all, rate, bias, direction, h, half):
    nx, nz, rows, _ = ctx_all.shape
    tokens = nx * nz * rows
    data = jnp.concatenate(
        [ctx_all[i, j].astype(F32) for j in range(nz) for i in range(nx)], axis=0
    )
    keys_all = unit_normal(silu(data[:, :HEAD]))
    values_all = silu(
        jnp.where(half == 0, data[:, HEAD : HEAD + HALF], data[:, HEAD + HALF : 2 * HEAD])
    )
    rates = data[:, 2 * HEAD :]
    lane = iota2(rates.shape, 1)
    mine = direction * HEADS_DEV + h
    decay_raw = jnp.sum(jnp.where(lane == mine, rates, 0.0), axis=1, keepdims=True)
    beta_raw = jnp.sum(jnp.where(lane == mine + CHAINS, rates, 0.0), axis=1, keepdims=True)
    log_decay = -rate * softplus(decay_raw + bias)
    betas = jax.nn.sigmoid(beta_raw) * (beta_scale * rate)
    row, col = iota2((BLOCK, BLOCK), 0), iota2((BLOCK, BLOCK), 1)
    flip = direction * (BLOCK - 1)
    sign = 1 - 2 * direction
    place = (flip + sign * row, flip + sign * col)
    tri = (place[0] >= place[1]).astype(F32)
    jobs, lows = [], []
    for b in range(tokens // BLOCK):
        part = slice(b * BLOCK, (b + 1) * BLOCK)
        sums = mm_full(tri, jnp.broadcast_to(log_decay[part], (BLOCK, HEAD)))[:, :1]
        final = jnp.sum(log_decay[part], axis=0, keepdims=True)
        keys, values = keys_all[part], values_all[part]
        gram = mm3(keys, keys, NT)
        low, right, decayed, _, _ = chain_terms(
            keys, values, gram, sums, final, betas[part], place
        )
        lows.append(low)
        jobs.append((right, decayed, final))
    steps = []
    for (right, decayed, final), inverse in zip(jobs, unit_inverses(lows, [place] * len(lows))):
        steps.append((mm1(decayed, mm3(inverse, right), TN), jnp.exp(final)))
    return steps


LOADED = [
    "cond",
    "ctx_cond",
    "w_mod",
    "latent",
    "context",
    "gain",
    "w_key",
    "w_value",
    "w_decay",
    "w_beta",
    "extra",
    "w_query",
    "w_outgate",
    "out_gain",
    "w_out",
    "rate",
    "bias",
]
IN_SMEM = ("rate", "bias")
COMM = ["mod1", "mod2", "ctx", "ctx2", "near", "far", "back", "tp"]


def whole_kernel(nz, nx, ny, hbm, out_ref, loads, load_sem, mem, send, recv):
    z, x, y = lax.axis_index(ZAX), lax.axis_index(XAX), lax.axis_index(YAX)
    span = loads["latent"].shape[1]
    ctx_rows = loads["context"].shape[1]
    blocks = span // BLOCK
    rows_out = span // ny
    inner = HEADS_DEV * HEAD
    low_z = lax.rem(z, 2)
    group = z // 2
    groups = nz // 2
    members = 2 * nx
    own_head, own_half, direction = x // 2, lax.rem(x, 2), low_z
    sign = 1 - 2 * direction

    across = [(dx, dy) for dx in range(nx) for dy in range(ny) if (dx, dy) != (0, 0)]
    across.sort(key=lambda at: -min(at[0], nx - at[0]) - min(at[1], ny - at[1]))
    close = [(dl, dx) for dl in range(2) for dx in range(nx) if (dl, dx) != (0, 0)]
    close.sort(key=lambda at: -at[0] - min(at[1], nx - at[1]))
    along = sorted(range(1, nz), key=lambda dz: -min(dz, nz - dz))

    def across_target(dx, dy):
        return {XAX: lax.rem(x + dx, nx), YAX: lax.rem(y + dy, ny)}

    def close_place(dl, dx):
        return lax.rem(low_z + dl, 2), lax.rem(x + dx, nx)

    barrier = pltpu.get_barrier_semaphore()
    peers = [{ZAX: lax.rem(z + dz, nz)} for dz in range(1, nz)]
    peers += [across_target(*at) for at in across]
    peers += [
        {ZAX: group * 2 + lax.rem(low_z + 1, 2), XAX: lax.rem(x + dx, nx)} for dx in range(1, nx)
    ]
    for target in peers:
        pl.semaphore_signal(barrier, inc=1, device_id=target, device_id_type=MESH)
    fetched = {}
    rate_ref, bias_ref = loads["rate"], loads["bias"]
    for i, name in enumerate(LOADED):
        fetched[name] = pltpu.make_async_copy(hbm[name], loads[name], load_sem.at[i])
        fetched[name].start()

    def remote(kind, k, source, destination, target):
        return pltpu.make_async_remote_copy(
            src_ref=source,
            dst_ref=destination,
            send_sem=send[kind].at[k],
            recv_sem=recv[kind].at[k],
            device_id=target,
            device_id_type=MESH,
        )

    started = []

    def begin(copy):
        copy.start()
        started.append(copy)
        return copy

    part, slots, spread = mem["part"], mem["mod_slots"], mem["spread"]
    width = part.shape[1]
    for name in ("cond", "ctx_cond", "w_mod"):
        fetched[name].wait()
    cond = jnp.concatenate(
        [loads["cond"][...].astype(F32), loads["ctx_cond"][...].astype(F32)], axis=0
    )
    part[...] = dot16(silu(cond).astype(BF16), loads["w_mod"][...])
    pl.semaphore_wait(barrier, len(peers))
    arriving = [
        begin(remote("mod1", dz, part, slots.at[dz], {ZAX: lax.rem(z + dz, nz)})) for dz in along
    ]
    for name in ("latent", "context", "gain"):
        fetched[name].wait()
    gain = jnp.concatenate(
        [loads["gain"][i : i + 1, :].astype(F32) for i in range(D // HEAD)], axis=1
    )

    def normed(values):
        values = values.astype(F32)
        mean = jnp.mean(values * values, axis=-1, keepdims=True)
        return values * lax.rsqrt(mean + norm_eps) * gain

    mem["normed"][:span, :] = normed(loads["latent"][0])
    mem["normed"][span : span + ctx_rows, :] = normed(loads["context"][0])

    summed = part[...]
    for dz, copy in reversed(list(zip(along, arriving))):
        copy.wait_recv()
        summed = summed + slots[dz]
    spread[y * nx + x] = summed
    arriving = [
        begin(
            remote(
                "mod2",
                dy * nx + dx,
                spread.at[y * nx + x],
                spread.at[y * nx + x],
                across_target(dx, dy),
            )
        )
        for dx, dy in across
    ]
    for name in ("w_key", "w_value", "w_decay", "w_beta", "extra", "rate", "bias"):
        fetched[name].wait()
    small = jnp.concatenate(
        [loads[name][d].astype(F32) for name in ("w_decay", "w_beta") for d in range(2)], axis=0
    ).astype(BF16)
    extra = jnp.concatenate([loads["extra"][0, d] for d in range(2)], axis=0)
    eye_span = (iota2((span, span), 0) == iota2((span, span), 1)).astype(F32)
    added = mm_full(eye_span, extra, NT)
    for copy in arriving:
        copy.wait_recv()
    mod = mem["mod"]
    for j in range(ny):
        summed = spread[j * nx]
        for i in range(1, nx):
            summed = summed + spread[j * nx + i]
        mod[:, j * width : (j + 1) * width] = summed

    rows = mem["rows"]
    rows[:span, :] = (
        mem["normed"][:span, :] * (1.0 + mod[0:1, D : 2 * D]) + mod[0:1, :D]
    ).astype(BF16)
    ctx_in = mem["normed"][span : span + ctx_rows, :] * (1.0 + mod[1:2, D : 2 * D]) + mod[1:2, :D]
    rows[span:, :] = jnp.concatenate(
        [ctx_in, jnp.zeros((rows.shape[0] - span - ctx_rows, D), F32)], axis=0
    ).astype(BF16)
    key_raw = round16(dot16(rows[...], loads["w_key"][...]))
    value_raw = round16(dot16(rows[...], loads["w_value"][...]))
    rates_raw = round16(dot16(rows[...], small, NT))

    ctx_z, ctx_all = mem["ctx_z"], mem["ctx_all"]
    ctx_rates = jnp.concatenate(
        [rates_raw[span : span + ctx_rows], jnp.zeros((ctx_rows, HEAD - 2 * CHAINS), F32)], axis=1
    )
    for h in range(HEADS_DEV):
        lanes = slice(h * HEAD, (h + 1) * HEAD)
        ctx_z[h, z] = jnp.concatenate(
            [
                key_raw[span : span + ctx_rows, lanes],
                value_raw[span : span + ctx_rows, lanes],
                ctx_rates,
            ],
            axis=1,
        ).astype(BF16)
    ctx_arriving = [
        begin(
            remote(
                "ctx",
                h * nz + dz,
                ctx_z.at[h, z],
                ctx_z.at[h, z],
                {ZAX: lax.rem(z + dz, nz)},
            )
        )
        for dz in along
        for h in range(HEADS_DEV)
    ]

    lane4 = iota2((1, CHAINS), 1)

    def by_lane(ref):
        line = jnp.zeros((1, CHAINS), F32)
        for d in range(2):
            for h in range(HEADS_DEV):
                line = jnp.where(lane4 == d * HEADS_DEV + h, ref[d, h], line)
        return line

    rate = by_lane(rate_ref)
    log_decay = -rate * softplus(rates_raw[:span, :CHAINS] + by_lane(bias_ref)) + added
    betas = jax.nn.sigmoid(rates_raw[:span, CHAINS:]) * (beta_scale * rate)
    row, col = iota2((BLOCK, BLOCK), 0), iota2((BLOCK, BLOCK), 1)
    places = [(row, col), (BLOCK - 1 - row, BLOCK - 1 - col)]
    tris = [(row >= col).astype(F32), (row <= col).astype(F32)]
    sums = [
        [mm_full(tris[d], log_decay[b * BLOCK : (b + 1) * BLOCK]) for b in range(blocks)]
        for d in range(2)
    ]
    jobs, lows, orders, key_parts = [], [], [], {}
    for h in range(HEADS_DEV):
        lanes = slice(h * HEAD, (h + 1) * HEAD)
        keys_h = unit_normal(silu(key_raw[:span, lanes]))
        values_h = silu(value_raw[:span, lanes])
        for b in range(blocks):
            at = slice(b * BLOCK, (b + 1) * BLOCK)
            keys, values = keys_h[at], values_h[at]
            key_parts[h, b] = keys
            gram = mm3(keys, keys, NT)
            for d in range(2):
                lane = d * HEADS_DEV + h
                cums = sums[d][b][:, lane : lane + 1]
                final = cums[BLOCK - 1 : BLOCK] if d == 0 else cums[0:1]
                low, right, decayed, weights, grown = chain_terms(
                    keys, values, gram, cums, final, betas[at, lane : lane + 1], places[d]
                )
                lows.append(low)
                orders.append(places[d])
                jobs.append((h, d, b, right, decayed, weights, grown, final))
    inverses = unit_inverses(lows, orders)
    found = {}
    for (h, d, b, right, decayed, weights, grown, final), inverse in zip(jobs, inverses):
        solved = mm3(inverse, right)
        step = mm1(decayed, solved, TN)
        found[h, d, b] = (-step[:, :HEAD], step[:, HEAD:], jnp.exp(final), solved, weights, grown)
    maps = mem["maps"]
    before = {}
    for h in range(HEADS_DEV):
        for d in range(2):
            whole = None
            for b in range(blocks) if d == 0 else reversed(range(blocks)):
                near, offset, decay = found[h, d, b][:3]
                before[h, d, b] = whole
                if whole is None:
                    whole = (decay, near, offset)
                else:
                    decay_all, near_all, offset_all = whole
                    moved = mm1(near, jnp.concatenate([near_all, offset_all], axis=1))
                    whole = (
                        decay * decay_all,
                        decay * near_all + decay_all * near + moved[:, :HEAD],
                        decay * offset_all + moved[:, HEAD:] + offset,
                    )
            decay, near, offset = whole
            for c in range(2):
                index = (2 * h + d) * 2 + c
                put_map(maps, index, decay, near, offset[:, c * HALF : (c + 1) * HALF])

    near_slots = mem["near_slots"]

    def map_index(low, at_x):
        return ((at_x // 2) * 2 + low) * 2 + lax.rem(at_x, 2)

    near_slots[0] = maps[map_index(low_z, x)]
    arriving = []
    for dl, dx in close:
        low, at_x = close_place(dl, dx)
        arriving.append(
            begin(
                remote(
                    "near",
                    dl * nx + dx,
                    maps.at[map_index(low, at_x)],
                    near_slots.at[dl * nx + dx],
                    {ZAX: group * 2 + low, XAX: at_x},
                )
            )
        )

    for copy in ctx_arriving:
        copy.wait_recv()
    ctx_all[x] = ctx_z[own_head]
    ctx_arriving = []
    for dx in range(1, nx):
        to = lax.rem(x + dx, nx)
        ctx_arriving.append(
            begin(remote("ctx2", dx, ctx_z.at[to // 2], ctx_all.at[x], {XAX: to}))
        )

    for name in ("w_query", "w_outgate", "out_gain"):
        fetched[name].wait()
    query_raw = round16(dot16(rows[:span, :], loads["w_query"][...]))
    mem["gate"][...] = silu(round16(dot16(rows[:span, :], loads["w_outgate"][...])))
    reads, base = mem["reads"], mem["base"]
    for h in range(HEADS_DEV):
        lanes = slice(h * HEAD, (h + 1) * HEAD)
        queries_h = unit_normal(silu(query_raw[:, lanes])) * HEAD ** (-0.5)
        for b in range(blocks):
            at = slice(b * BLOCK, (b + 1) * BLOCK)
            queries = queries_h[at]
            cross = mm1(queries, key_parts[h, b], NT)
            fixed = None
            for d in range(2):
                _, _, _, solved, weights, grown = found[h, d, b]
                read = mm1(cross * weights, solved)
                reader = queries * grown - read[:, :HEAD]
                now = read[:, HEAD:]
                to = slice(d * HEAD, (d + 1) * HEAD)
                if before[h, d, b] is None:
                    reads[h, at, to] = reader.astype(BF16)
                else:
                    decay_all, near_all, offset_all = before[h, d, b]
                    moved = mm1(reader, jnp.concatenate([near_all, offset_all], axis=1))
                    reads[h, at, to] = (decay_all * reader + moved[:, :HEAD]).astype(BF16)
                    now = now + moved[:, HEAD:]
                fixed = now if fixed is None else fixed + now
            base[h, at, :] = fixed

    for copy in arriving:
        copy.wait_recv()
    prefix_near, prefix_offset, prefix_decay = (
        mem["prefix_near"],
        mem["prefix_offset"],
        mem["prefix_decay"],
    )
    whole = None
    for p in range(members):
        source = p + direction * (members - 1 - 2 * p)
        from_low, from_x = source // nx, lax.rem(source, nx)
        slot = lax.rem(low_z - from_low + 2, 2) * nx + lax.rem(x - from_x + nx, nx)
        decay, near16, offset = get_map(near_slots, slot)
        near = near16.astype(F32)
        if whole is None:
            prefix_near[0] = jnp.zeros((HEAD, HEAD), BF16)
            prefix_offset[0] = jnp.zeros((HEAD, HALF), F32)
            prefix_decay[0] = jnp.ones((8, HALF), F32)
            whole = (decay, near, offset)
        else:
            decay_all, near_all, offset_all = whole
            prefix_near[p] = near_all.astype(BF16)
            prefix_offset[p] = offset_all
            prefix_decay[p] = jnp.broadcast_to(decay_all[:, :HALF], (8, HALF))
            moved = mm_exact_left(near16, jnp.concatenate([near_all, offset_all], axis=1))
            whole = (
                decay * decay_all,
                decay * near_all + decay_all * near + moved[:, :HEAD],
                decay[:, :HALF] * offset_all + moved[:, HEAD:] + offset,
            )
    put_map(mem["sending"], 0, *whole)
    far_slots = mem["far_slots"]

    def far_copy(k):
        return remote(
            "far",
            k,
            mem["sending"].at[0],
            far_slots.at[k],
            {ZAX: lax.rem(z + 2 * k * sign + nz, nz)},
        )

    behind = group + direction * (groups - 1 - 2 * group)
    ahead = groups - 1 - behind
    for k in sorted(range(1, groups), key=lambda k: -min(2 * k, nz - 2 * k)):

        @pl.when(k <= ahead)
        def _(k=k):
            far_copy(k).start()

    for copy in ctx_arriving:
        copy.wait_recv()
    steps = context_steps(
        ctx_all, rate_ref[direction, own_head], bias_ref[direction, own_head],
        direction, own_head, own_half,
    )
    ctx_steps, ctx_decay, state = mem["ctx_steps"], mem["ctx_decay"], mem["state"]
    for b, (step, decay) in enumerate(steps):
        ctx_steps[b] = step
        ctx_decay[b] = jnp.broadcast_to(decay, (8, HALF))
    first = direction * (len(steps) - 1)
    now = ctx_steps[first][:, HEAD:]
    for b in range(1, len(steps)):
        at = first + sign * b
        step = ctx_steps[at]
        now = ctx_decay[at, 0:1, :] * now - mm3(step[:, :HEAD], now) + step[:, HEAD:]
    state[...] = now
    for k in reversed(range(1, groups)):

        @pl.when(k <= behind)
        def _(k=k):
            far_copy(k).wait_recv()
            decay, near16, offset = get_map(far_slots, k)
            now = state[...]
            state[...] = decay[:, :HALF] * now + mm_exact_left(near16, now) + offset

    now = state[...]
    now16 = now.astype(BF16)

    def entering(low, at_x):
        place = low * nx + at_x
        p = place + direction * (members - 1 - 2 * place)
        values = prefix_decay[p, 0:1, :] * now + dot16(prefix_near[p], now16) + prefix_offset[p]
        return pack_halves(values).astype(BF16)

    leaving, states = mem["leaving"], mem["states"]
    mine = low_z * nx + x
    spots = [close_place(dl, dx) for dl, dx in close]
    states[mine] = entering(low_z, x)
    for at, values in zip(close, [entering(low, at_x) for low, at_x in spots]):
        leaving[at[0] * nx + at[1]] = values
    arriving = []
    for (dl, dx), (low, at_x) in zip(close, spots):
        k = dl * nx + dx
        arriving.append(
            begin(
                remote(
                    "back", k, leaving.at[k], states.at[mine], {ZAX: group * 2 + low, XAX: at_x}
                )
            )
        )
    for copy in arriving:
        copy.wait_recv()

    gated, gathered = mem["gated"], mem["gathered"]
    head_gain = loads["out_gain"][...].astype(F32)
    for h in range(HEADS_DEV):
        whole = jnp.concatenate(
            [
                jnp.concatenate(
                    [unpack_halves(states[d * nx + 2 * h + c].astype(F32)) for c in range(2)],
                    axis=1,
                )
                for d in range(2)
            ],
            axis=0,
        ).astype(BF16)
        total = dot16(reads[h], whole) + base[h]
        scaled = total * lax.rsqrt(jnp.mean(total * total, axis=-1, keepdims=True) + norm_eps)
        lanes = slice(h * HEAD, (h + 1) * HEAD)
        result = (scaled * head_gain * mem["gate"][:, lanes]).astype(BF16)
        for t in range(ny):
            gated[t, :, lanes] = result[t * rows_out : (t + 1) * rows_out]
    arriving = []
    for dy in range(1, ny):
        to = lax.rem(y + dy, ny)
        arriving.append(begin(remote("tp", dy, gated.at[to], gathered.at[dy], {YAX: to})))
    fetched["w_out"].wait()
    w_out = loads["w_out"]

    def product(values, owner):
        return dot16(values, w_out[pl.ds(pl.multiple_of(owner * inner, inner), inner), :])

    mixed = product(gated[y], y)
    for dy, copy in zip(range(1, ny), arriving):
        copy.wait_recv()
        mixed = mixed + product(gathered[dy], lax.rem(y - dy + ny, ny))
    own = loads["latent"][0, pl.ds(pl.multiple_of(y * rows_out, 16), rows_out), :].astype(F32)
    out_ref[...] = (own + mod[0:1, 2 * D :] * mixed).astype(BF16)

    for k in range(1, groups):

        @pl.when(k <= ahead)
        def _(k=k):
            far_copy(k).wait_send()

    for copy in started:
        copy.wait_send()


def whole(operands, nz, nx, ny):
    span, ctx_rows = operands["latent"].shape[1], operands["context"].shape[1]
    inner = HEADS_DEV * HEAD
    rows_out = span // ny
    width = operands["w_mod"].shape[1]
    members, groups = 2 * nx, nz // 2
    ctx_blocks = nz * nx * ctx_rows // BLOCK
    memory = {
        "part": ((2, width), F32),
        "mod_slots": ((nz, 2, width), F32),
        "spread": ((nx * ny, 2, width), F32),
        "mod": ((2, width * ny), F32),
        "normed": ((span + ctx_rows, D), F32),
        "rows": ((span + 16, D), BF16),
        "ctx_z": ((HEADS_DEV, nz, ctx_rows, 3 * HEAD), BF16),
        "ctx_all": ((nx, nz, ctx_rows, 3 * HEAD), BF16),
        "maps": ((2 * CHAINS, MAP_ROWS, HEAD), BF16),
        "near_slots": ((members, MAP_ROWS, HEAD), BF16),
        "gate": ((span, inner), F32),
        "reads": ((HEADS_DEV, span, 2 * HEAD), BF16),
        "base": ((HEADS_DEV, span, HEAD), F32),
        "prefix_near": ((members, HEAD, HEAD), BF16),
        "prefix_offset": ((members, HEAD, HALF), F32),
        "prefix_decay": ((members, 8, HALF), F32),
        "sending": ((1, MAP_ROWS, HEAD), BF16),
        "far_slots": ((groups, MAP_ROWS, HEAD), BF16),
        "ctx_steps": ((ctx_blocks, HEAD, HEAD + HALF), F32),
        "ctx_decay": ((ctx_blocks, 8, HALF), F32),
        "state": ((HEAD, HALF), F32),
        "leaving": ((members, HALF, HEAD), BF16),
        "states": ((members, HALF, HEAD), BF16),
        "gated": ((ny, rows_out, inner), BF16),
        "gathered": ((ny, rows_out, inner), BF16),
    }
    counts = {
        "mod1": nz,
        "mod2": nx * ny,
        "ctx": HEADS_DEV * nz,
        "ctx2": nx,
        "near": members,
        "far": groups,
        "back": members,
        "tp": ny,
    }

    def kernel(*refs):
        refs = list(refs)

        def take(names):
            return {name: refs.pop(0) for name in names}

        hbm = take(LOADED)
        out_ref = refs.pop(0)
        loads = take(LOADED)
        load_sem = refs.pop(0)
        mem = take(memory)
        send, recv = take(COMM), take(COMM)
        whole_kernel(
            nz, nx, ny, hbm, out_ref, loads, load_sem, mem, send, recv
        )

    return pl.pallas_call(
        kernel,
        out_shape=jax.ShapeDtypeStruct((rows_out, D), BF16),
        in_specs=[pl.BlockSpec(memory_space=pl.ANY)] * len(LOADED),
        out_specs=pl.BlockSpec(memory_space=pltpu.VMEM),
        scratch_shapes=[
            (pltpu.SMEM if n in IN_SMEM else pltpu.VMEM)(operands[n].shape, operands[n].dtype)
            for n in LOADED
        ]
        + [pltpu.SemaphoreType.DMA((len(LOADED),))]
        + [pltpu.VMEM(*memory[name]) for name in memory]
        + [pltpu.SemaphoreType.DMA((counts[name],)) for name in COMM + COMM],
        compiler_params=pltpu.CompilerParams(collective_id=0, has_side_effects=True),
        name="whole",
    )(*[operands[name] for name in LOADED])


def on_device(
    latent,
    cond,
    context,
    ctx_cond,
    w_mod,
    norm_gain,
    w_query,
    w_key,
    w_value,
    w_outgate,
    w_decay,
    w_beta,
    decay_rate,
    decay_bias,
    extra_decay,
    out_gain,
    w_out,
):
    operands = {
        "cond": cond,
        "ctx_cond": ctx_cond[None, :],
        "w_mod": w_mod,
        "latent": latent,
        "context": context,
        "gain": norm_gain.reshape(D // HEAD, HEAD),
        "w_key": w_key,
        "w_value": w_value,
        "w_decay": jnp.transpose(w_decay, (1, 2, 0)),
        "w_beta": jnp.transpose(w_beta, (1, 2, 0)),
        "extra": extra_decay,
        "w_query": w_query,
        "w_outgate": w_outgate,
        "out_gain": out_gain[None, :],
        "w_out": w_out,
        "rate": decay_rate,
        "bias": decay_bias,
    }
    sizes = [lax.axis_size(name) for name in (ZAX, XAX, YAX)]
    return whole(operands, *sizes)[None]


def solution(mesh):
    torus = Mesh(
        mesh.devices.reshape(-1, 4, mesh.shape["tp"], mesh.shape["dp"]), (ZAX, XAX, YAX, "dp")
    )
    return jax.shard_map(
        on_device,
        mesh=torus,
        in_specs=(
            P("dp", SP, None),
            P("dp", SP),
            P("dp", SP, None),
            P(SP),
            P(SP, "tp"),
            P(),
            P(None, "tp"),
            P(None, "tp"),
            P(None, "tp"),
            P(None, "tp"),
            P(None, None, "tp"),
            P(None, None, "tp"),
            P(None, "tp"),
            P(None, "tp"),
            P("dp", None, "tp", SP),
            P(),
            P(),
        ),
        out_specs=P("dp", SP_TP, None),
        check_vma=False,
    )
```

```python
import functools

import jax
import jax.numpy as jnp
from jax import lax
from jax.experimental import pallas as pl
from jax.experimental.pallas import tpu as pltpu
from jax.sharding import Mesh
from jax.sharding import PartitionSpec as P

D = 2048
HEAD = 128
BLOCK = 64
HEADS_DEV = 2
CHAINS = 2 * HEADS_DEV
HALF = HEAD // 2
MAP_ROWS = HEAD + HALF + 16
ZAX, XAX, YAX = "sp_0", "sp_1", "tp"
SP = (ZAX, XAX)
SP_TP = (ZAX, XAX, YAX)
MESH = pl.DeviceIdType.MESH
F32 = jnp.float32
BF16 = jnp.bfloat16

norm_eps = 1e-06
beta_scale = 30.0

NN = (((1,), (0,)), ((), ()))
NT = (((1,), (1,)), ((), ()))
TN = (((0,), (0,)), ((), ()))


def dot16(left, right, dims=NN):
    return lax.dot_general(left, right, dims, preferred_element_type=F32)


def mm1(left, right, dims=NN):
    return dot16(left.astype(BF16), right.astype(BF16), dims)


def halves(values):
    high = values.astype(BF16)
    return high, (values - high.astype(F32)).astype(BF16)


def mm3(left, right, dims=NN):
    left_high, left_low = halves(left)
    right_high, right_low = halves(right)
    return dot16(left_high, right_high, dims) + (
        dot16(left_high, right_low, dims) + dot16(left_low, right_high, dims)
    )


def mm_exact_left(left, right, dims=NN):
    high, low = halves(right)
    left = left.astype(BF16)
    return dot16(left, high, dims) + dot16(left, low, dims)


def mm_full(left, right, dims=NN):
    return lax.dot_general(
        left, right, dims, preferred_element_type=F32, precision=lax.Precision.HIGHEST
    )


def silu(values):
    return values * jax.nn.sigmoid(values)


def softplus(values):
    return jnp.maximum(values, 0.0) + jnp.log1p(jnp.exp(-jnp.abs(values)))


def unit_normal(values):
    return values * lax.rsqrt(jnp.sum(values * values, axis=-1, keepdims=True) + norm_eps)


def iota2(shape, dim):
    return lax.broadcasted_iota(jnp.int32, shape, dim)


def unit_inverses(lows, places):
    eye = (iota2((BLOCK, BLOCK), 0) == iota2((BLOCK, BLOCK), 1)).astype(F32)

    def coupling(low, place, level):
        row, col = place
        joined = (row >> (level + 1)) == (col >> (level + 1))
        mask = joined & (((row >> level) & 1) == 1) & (((col >> level) & 1) == 0)
        return jnp.where(mask, low, 0.0)

    results = [eye - coupling(low, place, 0) for low, place in zip(lows, places)]
    for level in range(1, (BLOCK - 1).bit_length()):
        inner = [
            mm3(coupling(low, place, level), result)
            for low, place, result in zip(lows, places, results)
        ]
        results = [result - mm3(result, term) for result, term in zip(results, inner)]
    return results


def chain_terms(keys, values, gram, sums, final, betas, place):
    row, col = place
    eye = iota2((BLOCK, BLOCK), 0) == iota2((BLOCK, BLOCK), 1)
    wide = jnp.broadcast_to(sums, (BLOCK, BLOCK))
    across = jnp.sum(jnp.where(eye, wide, 0.0), axis=0, keepdims=True)
    lower = row >= col
    weights = jnp.where(lower, jnp.exp(jnp.where(lower, wide - across, 0.0)), 0.0)
    low = jnp.where(row > col, gram * betas * weights, 0.0)
    grown = jnp.exp(sums)
    scaled = keys * betas
    right = jnp.concatenate([scaled * grown, values * betas], axis=1)
    decayed = keys * jnp.exp(final - sums)
    return low, right, decayed, weights, grown


def round16(values):
    return values.astype(BF16).astype(F32)


def pack_halves(values):
    return jnp.concatenate([values[: HEAD // 2], values[HEAD // 2 :]], axis=1)


def unpack_halves(values):
    return jnp.concatenate([values[:, : HEAD // 2], values[:, HEAD // 2 :]], axis=0)


def decay_rows(decay):
    high = round16(decay)
    middle = round16(decay - high)
    last = decay - high - middle
    row = iota2((16, HEAD), 0)
    pieces = jnp.where(row == 0, high, jnp.where(row == 1, middle, last))
    return jnp.where(row < 3, pieces, 0.0).astype(BF16)


def put_map(ref, index, decay, near, offset):
    ref[index, :HEAD, :] = near.astype(BF16)
    ref[index, HEAD : HEAD + HALF, :] = pack_halves(offset).astype(BF16)
    ref[index, HEAD + HALF :, :] = decay_rows(decay)


def get_map(ref, index):
    pieces = ref[index, HEAD + HALF :, :].astype(F32)
    decay = pieces[0:1] + pieces[1:2] + pieces[2:3]
    offset = unpack_halves(ref[index, HEAD : HEAD + HALF, :].astype(F32))
    return decay, ref[index, :HEAD, :], offset


def context_steps(ctx_all, rate, bias, direction, h, half):
    nx, nz, rows, _ = ctx_all.shape
    tokens = nx * nz * rows
    data = jnp.concatenate(
        [ctx_all[i, j].astype(F32) for j in range(nz) for i in range(nx)], axis=0
    )
    keys_all = unit_normal(silu(data[:, :HEAD]))
    values_all = silu(
        jnp.where(half == 0, data[:, HEAD : HEAD + HALF], data[:, HEAD + HALF : 2 * HEAD])
    )
    rates = data[:, 2 * HEAD :]
    lane = iota2(rates.shape, 1)
    mine = direction * HEADS_DEV + h
    decay_raw = jnp.sum(jnp.where(lane == mine, rates, 0.0), axis=1, keepdims=True)
    beta_raw = jnp.sum(jnp.where(lane == mine + CHAINS, rates, 0.0), axis=1, keepdims=True)
    log_decay = -rate * softplus(decay_raw + bias)
    betas = jax.nn.sigmoid(beta_raw) * (beta_scale * rate)
    row, col = iota2((BLOCK, BLOCK), 0), iota2((BLOCK, BLOCK), 1)
    flip = direction * (BLOCK - 1)
    sign = 1 - 2 * direction
    place = (flip + sign * row, flip + sign * col)
    tri = (place[0] >= place[1]).astype(F32)
    jobs, lows = [], []
    for b in range(tokens // BLOCK):
        part = slice(b * BLOCK, (b + 1) * BLOCK)
        sums = mm_full(tri, jnp.broadcast_to(log_decay[part], (BLOCK, HEAD)))[:, :1]
        final = jnp.sum(log_decay[part], axis=0, keepdims=True)
        keys, values = keys_all[part], values_all[part]
        gram = mm3(keys, keys, NT)
        low, right, decayed, _, _ = chain_terms(
            keys, values, gram, sums, final, betas[part], place
        )
        lows.append(low)
        jobs.append((right, decayed, final))
    steps = []
    for (right, decayed, final), inverse in zip(jobs, unit_inverses(lows, [place] * len(lows))):
        steps.append((mm1(decayed, mm3(inverse, right), TN), jnp.exp(final)))
    return steps


LOADED = [
    "cond",
    "ctx_cond",
    "w_mod",
    "latent",
    "context",
    "gain",
    "w_key",
    "w_value",
    "w_decay",
    "w_beta",
    "extra",
    "w_query",
    "w_outgate",
    "out_gain",
    "w_out",
    "rate",
    "bias",
]
IN_SMEM = ("rate", "bias")
COMM = ["mod1", "mod2", "ctx", "ctx2", "near", "far", "back", "tp"]


def whole_kernel(nz, nx, ny, hbm, out_ref, loads, load_sem, mem, send, recv, ready):
    z, x, y = lax.axis_index(ZAX), lax.axis_index(XAX), lax.axis_index(YAX)
    span = loads["latent"].shape[1]
    ctx_rows = loads["context"].shape[1]
    blocks = span // BLOCK
    rows_out = span // ny
    inner = HEADS_DEV * HEAD
    low_z = lax.rem(z, 2)
    group = z // 2
    groups = nz // 2
    members = 2 * nx
    own_head, own_half, direction = x // 2, lax.rem(x, 2), low_z
    sign = 1 - 2 * direction

    across = [(dx, dy) for dx in range(nx) for dy in range(ny) if (dx, dy) != (0, 0)]
    across.sort(key=lambda at: -min(at[0], nx - at[0]) - min(at[1], ny - at[1]))
    close = [(dl, dx) for dl in range(2) for dx in range(nx) if (dl, dx) != (0, 0)]
    close.sort(key=lambda at: -at[0] - min(at[1], nx - at[1]))
    along = sorted(range(1, nz), key=lambda dz: -min(dz, nz - dz))

    def across_target(dx, dy):
        return {XAX: lax.rem(x + dx, nx), YAX: lax.rem(y + dy, ny)}

    def close_place(dl, dx):
        return lax.rem(low_z + dl, 2), lax.rem(x + dx, nx)

    barrier = pltpu.get_barrier_semaphore()
    peers = [{ZAX: lax.rem(z + dz, nz)} for dz in range(1, nz)]
    peers += [{XAX: lax.rem(x + dx, nx)} for dx in range(1, nx)]
    peers += [{YAX: lax.rem(y + dy, ny)} for dy in range(1, ny)]
    for target in peers:
        pl.semaphore_signal(barrier, inc=1, device_id=target, device_id_type=MESH)
    fetched = {}
    rate_ref, bias_ref = loads["rate"], loads["bias"]
    for i, name in enumerate(LOADED):
        fetched[name] = pltpu.make_async_copy(hbm[name], loads[name], load_sem.at[i])
        fetched[name].start()

    def remote(kind, k, source, destination, target):
        return pltpu.make_async_remote_copy(
            src_ref=source,
            dst_ref=destination,
            send_sem=send[kind].at[k],
            recv_sem=recv[kind].at[k],
            device_id=target,
            device_id_type=MESH,
        )

    started = []

    def begin(copy):
        copy.start()
        started.append(copy)
        return copy

    def sends_done():
        while started:
            started.pop(0).wait_send()

    part, slots, spread = mem["part"], mem["mod_slots"], mem["spread"]
    width = part.shape[1]
    for name in ("cond", "ctx_cond", "w_mod"):
        fetched[name].wait()
    cond = jnp.concatenate(
        [loads["cond"][...].astype(F32), loads["ctx_cond"][...].astype(F32)], axis=0
    )
    part[...] = dot16(silu(cond).astype(BF16), loads["w_mod"][...])
    pl.semaphore_wait(barrier, len(peers))
    arriving = [
        begin(remote("mod1", dz, part, slots.at[dz], {ZAX: lax.rem(z + dz, nz)})) for dz in along
    ]
    for dx in range(1, nx):
        pl.semaphore_signal(
            ready.at[0], inc=1, device_id={XAX: lax.rem(x + dx, nx)}, device_id_type=MESH
        )
    pl.semaphore_signal(
        ready.at[1],
        inc=1,
        device_id={ZAX: group * 2 + lax.rem(low_z + 1, 2)},
        device_id_type=MESH,
    )
    for name in ("latent", "context", "gain"):
        fetched[name].wait()
    gain = jnp.concatenate(
        [loads["gain"][i : i + 1, :].astype(F32) for i in range(D // HEAD)], axis=1
    )

    def normed(values):
        values = values.astype(F32)
        mean = jnp.mean(values * values, axis=-1, keepdims=True)
        return values * lax.rsqrt(mean + norm_eps) * gain

    mem["normed"][:span, :] = normed(loads["latent"][0])
    mem["normed"][span : span + ctx_rows, :] = normed(loads["context"][0])

    summed = part[...]
    for dz, copy in reversed(list(zip(along, arriving))):
        copy.wait_recv()
        summed = summed + slots[dz]
    spread[y * nx + x] = summed
    pl.semaphore_wait(ready.at[0], nx - 1)
    arriving = [
        begin(
            remote(
                "mod2",
                dy * nx + dx,
                spread.at[y * nx + x],
                spread.at[y * nx + x],
                across_target(dx, dy),
            )
        )
        for dx, dy in across
    ]
    for name in ("w_key", "w_value", "w_decay", "w_beta", "extra", "rate", "bias"):
        fetched[name].wait()
    small = jnp.concatenate(
        [loads[name][d].astype(F32) for name in ("w_decay", "w_beta") for d in range(2)], axis=0
    ).astype(BF16)
    extra = jnp.concatenate([loads["extra"][0, d] for d in range(2)], axis=0)
    eye_span = (iota2((span, span), 0) == iota2((span, span), 1)).astype(F32)
    added = mm_full(eye_span, extra, NT)
    for copy in arriving:
        copy.wait_recv()
    mod = mem["mod"]
    for j in range(ny):
        summed = spread[j * nx]
        for i in range(1, nx):
            summed = summed + spread[j * nx + i]
        mod[:, j * width : (j + 1) * width] = summed

    rows = mem["rows"]
    rows[:span, :] = (
        mem["normed"][:span, :] * (1.0 + mod[0:1, D : 2 * D]) + mod[0:1, :D]
    ).astype(BF16)
    ctx_in = mem["normed"][span : span + ctx_rows, :] * (1.0 + mod[1:2, D : 2 * D]) + mod[1:2, :D]
    rows[span:, :] = jnp.concatenate(
        [ctx_in, jnp.zeros((rows.shape[0] - span - ctx_rows, D), F32)], axis=0
    ).astype(BF16)
    key_raw = round16(dot16(rows[...], loads["w_key"][...]))
    value_raw = round16(dot16(rows[...], loads["w_value"][...]))
    rates_raw = round16(dot16(rows[...], small, NT))

    ctx_z, ctx_all = mem["ctx_z"], mem["ctx_all"]
    ctx_rates = jnp.concatenate(
        [rates_raw[span : span + ctx_rows], jnp.zeros((ctx_rows, HEAD - 2 * CHAINS), F32)], axis=1
    )
    for h in range(HEADS_DEV):
        lanes = slice(h * HEAD, (h + 1) * HEAD)
        ctx_z[h, z] = jnp.concatenate(
            [
                key_raw[span : span + ctx_rows, lanes],
                value_raw[span : span + ctx_rows, lanes],
                ctx_rates,
            ],
            axis=1,
        ).astype(BF16)
    ctx_arriving = [
        begin(
            remote(
                "ctx",
                h * nz + dz,
                ctx_z.at[h, z],
                ctx_z.at[h, z],
                {ZAX: lax.rem(z + dz, nz)},
            )
        )
        for dz in along
        for h in range(HEADS_DEV)
    ]

    lane4 = iota2((1, CHAINS), 1)

    def by_lane(ref):
        line = jnp.zeros((1, CHAINS), F32)
        for d in range(2):
            for h in range(HEADS_DEV):
                line = jnp.where(lane4 == d * HEADS_DEV + h, ref[d, h], line)
        return line

    rate = by_lane(rate_ref)
    log_decay = -rate * softplus(rates_raw[:span, :CHAINS] + by_lane(bias_ref)) + added
    betas = jax.nn.sigmoid(rates_raw[:span, CHAINS:]) * (beta_scale * rate)
    row, col = iota2((BLOCK, BLOCK), 0), iota2((BLOCK, BLOCK), 1)
    places = [(row, col), (BLOCK - 1 - row, BLOCK - 1 - col)]
    tris = [(row >= col).astype(F32), (row <= col).astype(F32)]
    sums = [
        [mm_full(tris[d], log_decay[b * BLOCK : (b + 1) * BLOCK]) for b in range(blocks)]
        for d in range(2)
    ]
    jobs, lows, orders, key_parts = [], [], [], {}
    for h in range(HEADS_DEV):
        lanes = slice(h * HEAD, (h + 1) * HEAD)
        keys_h = unit_normal(silu(key_raw[:span, lanes]))
        values_h = silu(value_raw[:span, lanes])
        for b in range(blocks):
            at = slice(b * BLOCK, (b + 1) * BLOCK)
            keys, values = keys_h[at], values_h[at]
            key_parts[h, b] = keys
            gram = mm3(keys, keys, NT)
            for d in range(2):
                lane = d * HEADS_DEV + h
                cums = sums[d][b][:, lane : lane + 1]
                final = cums[BLOCK - 1 : BLOCK] if d == 0 else cums[0:1]
                low, right, decayed, weights, grown = chain_terms(
                    keys, values, gram, cums, final, betas[at, lane : lane + 1], places[d]
                )
                lows.append(low)
                orders.append(places[d])
                jobs.append((h, d, b, right, decayed, weights, grown, final))
    inverses = unit_inverses(lows, orders)
    found = {}
    for (h, d, b, right, decayed, weights, grown, final), inverse in zip(jobs, inverses):
        solved = mm3(inverse, right)
        step = mm1(decayed, solved, TN)
        found[h, d, b] = (-step[:, :HEAD], step[:, HEAD:], jnp.exp(final), solved, weights, grown)
    maps = mem["maps"]
    before = {}
    for h in range(HEADS_DEV):
        for d in range(2):
            whole = None
            for b in range(blocks) if d == 0 else reversed(range(blocks)):
                near, offset, decay = found[h, d, b][:3]
                before[h, d, b] = whole
                if whole is None:
                    whole = (decay, near, offset)
                else:
                    decay_all, near_all, offset_all = whole
                    moved = mm1(near, jnp.concatenate([near_all, offset_all], axis=1))
                    whole = (
                        decay * decay_all,
                        decay * near_all + decay_all * near + moved[:, :HEAD],
                        decay * offset_all + moved[:, HEAD:] + offset,
                    )
            decay, near, offset = whole
            for c in range(2):
                index = (2 * h + d) * 2 + c
                put_map(maps, index, decay, near, offset[:, c * HALF : (c + 1) * HALF])

    near_slots = mem["near_slots"]

    def map_index(low, at_x):
        return ((at_x // 2) * 2 + low) * 2 + lax.rem(at_x, 2)

    near_slots[0] = maps[map_index(low_z, x)]
    pl.semaphore_wait(ready.at[1], 1)
    arriving = []
    for dl, dx in close:
        low, at_x = close_place(dl, dx)
        arriving.append(
            begin(
                remote(
                    "near",
                    dl * nx + dx,
                    maps.at[map_index(low, at_x)],
                    near_slots.at[dl * nx + dx],
                    {ZAX: group * 2 + low, XAX: at_x},
                )
            )
        )

    for copy in ctx_arriving:
        copy.wait_recv()
    ctx_all[x] = ctx_z[own_head]
    ctx_arriving = []
    for dx in range(1, nx):
        to = lax.rem(x + dx, nx)
        ctx_arriving.append(
            begin(remote("ctx2", dx, ctx_z.at[to // 2], ctx_all.at[x], {XAX: to}))
        )

    for name in ("w_query", "w_outgate", "out_gain"):
        fetched[name].wait()
    query_raw = round16(dot16(rows[:span, :], loads["w_query"][...]))
    mem["gate"][...] = silu(round16(dot16(rows[:span, :], loads["w_outgate"][...])))
    reads, base = mem["reads"], mem["base"]
    for h in range(HEADS_DEV):
        lanes = slice(h * HEAD, (h + 1) * HEAD)
        queries_h = unit_normal(silu(query_raw[:, lanes])) * HEAD ** (-0.5)
        for b in range(blocks):
            at = slice(b * BLOCK, (b + 1) * BLOCK)
            queries = queries_h[at]
            cross = mm1(queries, key_parts[h, b], NT)
            fixed = None
            for d in range(2):
                _, _, _, solved, weights, grown = found[h, d, b]
                read = mm1(cross * weights, solved)
                reader = queries * grown - read[:, :HEAD]
                now = read[:, HEAD:]
                to = slice(d * HEAD, (d + 1) * HEAD)
                if before[h, d, b] is None:
                    reads[h, at, to] = reader.astype(BF16)
                else:
                    decay_all, near_all, offset_all = before[h, d, b]
                    moved = mm1(reader, jnp.concatenate([near_all, offset_all], axis=1))
                    reads[h, at, to] = (decay_all * reader + moved[:, :HEAD]).astype(BF16)
                    now = now + moved[:, HEAD:]
                fixed = now if fixed is None else fixed + now
            base[h, at, :] = fixed

    for copy in arriving:
        copy.wait_recv()
    prefix_near, prefix_offset, prefix_decay = (
        mem["prefix_near"],
        mem["prefix_offset"],
        mem["prefix_decay"],
    )
    def joined(later, earlier, exact):
        decay, near, offset = later
        decay_all, near_all, offset_all = earlier
        both = jnp.concatenate([near_all, offset_all], axis=1)
        moved = mm_exact_left(near, both) if exact else mm3(near, both)
        return (
            decay * decay_all,
            decay * near_all + decay_all * near + moved[:, :HEAD],
            decay[:, :HALF] * offset_all + moved[:, HEAD:] + offset,
        )

    single = []
    for p in range(members):
        source = p + direction * (members - 1 - 2 * p)
        from_low, from_x = source // nx, lax.rem(source, nx)
        slot = lax.rem(low_z - from_low + 2, 2) * nx + lax.rem(x - from_x + nx, nx)
        decay, near, offset = get_map(near_slots, slot)
        single.append((decay, near.astype(F32), offset))
    pairs = [joined(single[p + 1], single[p], True) for p in range(0, members, 2)]
    fours = [joined(pairs[p + 1], pairs[p], False) for p in range(0, members // 2, 2)]
    put_map(mem["sending"], 0, *joined(fours[1], fours[0], False))
    far_slots = mem["far_slots"]

    def far_copy(k):
        return remote(
            "far",
            k,
            mem["sending"].at[0],
            far_slots.at[k],
            {ZAX: lax.rem(z + 2 * k * sign + nz, nz)},
        )

    behind = group + direction * (groups - 1 - 2 * group)
    ahead = groups - 1 - behind
    for k in sorted(range(1, groups), key=lambda k: -min(2 * k, nz - 2 * k)):

        @pl.when(k <= ahead)
        def _(k=k):
            far_copy(k).start()

    third = joined(pairs[2], fours[0], False)
    prefixes = [
        single[0],
        pairs[0],
        joined(single[2], pairs[0], True),
        fours[0],
        joined(single[4], fours[0], True),
        third,
        joined(single[6], third, True),
    ]
    prefix_near[0] = jnp.zeros((HEAD, HEAD), BF16)
    prefix_offset[0] = jnp.zeros((HEAD, HALF), F32)
    prefix_decay[0] = jnp.ones((8, HALF), F32)
    for p, (decay, near, offset) in enumerate(prefixes):
        prefix_near[p + 1] = near.astype(BF16)
        prefix_offset[p + 1] = offset
        prefix_decay[p + 1] = jnp.broadcast_to(decay[:, :HALF], (8, HALF))
    sends_done()
    for copy in ctx_arriving:
        copy.wait_recv()
    steps = context_steps(
        ctx_all, rate_ref[direction, own_head], bias_ref[direction, own_head],
        direction, own_head, own_half,
    )
    ctx_steps, ctx_decay, state = mem["ctx_steps"], mem["ctx_decay"], mem["state"]
    for b, (step, decay) in enumerate(steps):
        ctx_steps[b] = step
        ctx_decay[b] = jnp.broadcast_to(decay, (8, HALF))
    first = direction * (len(steps) - 1)
    now = ctx_steps[first][:, HEAD:]
    for b in range(1, len(steps)):
        at = first + sign * b
        step = ctx_steps[at]
        now = ctx_decay[at, 0:1, :] * now - mm3(step[:, :HEAD], now) + step[:, HEAD:]
    state[...] = now
    for k in reversed(range(1, groups)):

        @pl.when(k <= behind)
        def _(k=k):
            far_copy(k).wait_recv()
            decay, near16, offset = get_map(far_slots, k)
            now = state[...]
            state[...] = decay[:, :HALF] * now + mm_exact_left(near16, now) + offset

    now = state[...]
    now16 = now.astype(BF16)

    def entering(low, at_x):
        place = low * nx + at_x
        p = place + direction * (members - 1 - 2 * place)
        values = prefix_decay[p, 0:1, :] * now + dot16(prefix_near[p], now16) + prefix_offset[p]
        return pack_halves(values).astype(BF16)

    leaving, states = mem["leaving"], mem["states"]
    mine = low_z * nx + x
    spots = [close_place(dl, dx) for dl, dx in close]
    states[mine] = entering(low_z, x)
    for at, values in zip(close, [entering(low, at_x) for low, at_x in spots]):
        leaving[at[0] * nx + at[1]] = values
    arriving = []
    for (dl, dx), (low, at_x) in zip(close, spots):
        k = dl * nx + dx
        arriving.append(
            begin(
                remote(
                    "back", k, leaving.at[k], states.at[mine], {ZAX: group * 2 + low, XAX: at_x}
                )
            )
        )
    for k in range(1, groups):

        @pl.when(k <= ahead)
        def _(k=k):
            far_copy(k).wait_send()

    for copy in arriving:
        copy.wait_recv()

    gated, gathered = mem["gated"], mem["gathered"]
    head_gain = loads["out_gain"][...].astype(F32)
    for h in range(HEADS_DEV):
        whole = jnp.concatenate(
            [
                jnp.concatenate(
                    [unpack_halves(states[d * nx + 2 * h + c].astype(F32)) for c in range(2)],
                    axis=1,
                )
                for d in range(2)
            ],
            axis=0,
        ).astype(BF16)
        total = dot16(reads[h], whole) + base[h]
        scaled = total * lax.rsqrt(jnp.mean(total * total, axis=-1, keepdims=True) + norm_eps)
        lanes = slice(h * HEAD, (h + 1) * HEAD)
        result = (scaled * head_gain * mem["gate"][:, lanes]).astype(BF16)
        for t in range(ny):
            gated[t, :, lanes] = result[t * rows_out : (t + 1) * rows_out]
    arriving = []
    for dy in range(1, ny):
        to = lax.rem(y + dy, ny)
        arriving.append(begin(remote("tp", dy, gated.at[to], gathered.at[dy], {YAX: to})))
    fetched["w_out"].wait()
    w_out = loads["w_out"]

    def product(values, owner):
        return dot16(values, w_out[pl.ds(pl.multiple_of(owner * inner, inner), inner), :])

    mixed = product(gated[y], y)
    for copy in started[:-(ny - 1)]:
        copy.wait_send()
    del started[: -(ny - 1)]
    for dy, copy in zip(range(1, ny), arriving):
        copy.wait_recv()
        mixed = mixed + product(gathered[dy], lax.rem(y - dy + ny, ny))
    own = loads["latent"][0, pl.ds(pl.multiple_of(y * rows_out, 16), rows_out), :].astype(F32)
    out_ref[...] = (own + mod[0:1, 2 * D :] * mixed).astype(BF16)

    sends_done()


def whole(operands, nz, nx, ny):
    span, ctx_rows = operands["latent"].shape[1], operands["context"].shape[1]
    inner = HEADS_DEV * HEAD
    rows_out = span // ny
    width = operands["w_mod"].shape[1]
    members, groups = 2 * nx, nz // 2
    ctx_blocks = nz * nx * ctx_rows // BLOCK
    memory = {
        "part": ((2, width), F32),
        "mod_slots": ((nz, 2, width), F32),
        "spread": ((nx * ny, 2, width), F32),
        "mod": ((2, width * ny), F32),
        "normed": ((span + ctx_rows, D), F32),
        "rows": ((span + 16, D), BF16),
        "ctx_z": ((HEADS_DEV, nz, ctx_rows, 3 * HEAD), BF16),
        "ctx_all": ((nx, nz, ctx_rows, 3 * HEAD), BF16),
        "maps": ((2 * CHAINS, MAP_ROWS, HEAD), BF16),
        "near_slots": ((members, MAP_ROWS, HEAD), BF16),
        "gate": ((span, inner), F32),
        "reads": ((HEADS_DEV, span, 2 * HEAD), BF16),
        "base": ((HEADS_DEV, span, HEAD), F32),
        "prefix_near": ((members, HEAD, HEAD), BF16),
        "prefix_offset": ((members, HEAD, HALF), F32),
        "prefix_decay": ((members, 8, HALF), F32),
        "sending": ((1, MAP_ROWS, HEAD), BF16),
        "far_slots": ((groups, MAP_ROWS, HEAD), BF16),
        "ctx_steps": ((ctx_blocks, HEAD, HEAD + HALF), F32),
        "ctx_decay": ((ctx_blocks, 8, HALF), F32),
        "state": ((HEAD, HALF), F32),
        "leaving": ((members, HALF, HEAD), BF16),
        "states": ((members, HALF, HEAD), BF16),
        "gated": ((ny, rows_out, inner), BF16),
        "gathered": ((ny, rows_out, inner), BF16),
    }
    counts = {
        "mod1": nz,
        "mod2": nx * ny,
        "ctx": HEADS_DEV * nz,
        "ctx2": nx,
        "near": members,
        "far": groups,
        "back": members,
        "tp": ny,
    }

    def kernel(*refs):
        refs = list(refs)

        def take(names):
            return {name: refs.pop(0) for name in names}

        hbm = take(LOADED)
        out_ref = refs.pop(0)
        loads = take(LOADED)
        load_sem = refs.pop(0)
        mem = take(memory)
        send, recv = take(COMM), take(COMM)
        whole_kernel(
            nz, nx, ny, hbm, out_ref, loads, load_sem, mem, send, recv, refs.pop(0)
        )

    return pl.pallas_call(
        kernel,
        out_shape=jax.ShapeDtypeStruct((rows_out, D), BF16),
        in_specs=[pl.BlockSpec(memory_space=pl.ANY)] * len(LOADED),
        out_specs=pl.BlockSpec(memory_space=pltpu.VMEM),
        scratch_shapes=[
            (pltpu.SMEM if n in IN_SMEM else pltpu.VMEM)(operands[n].shape, operands[n].dtype)
            for n in LOADED
        ]
        + [pltpu.SemaphoreType.DMA((len(LOADED),))]
        + [pltpu.VMEM(*memory[name]) for name in memory]
        + [pltpu.SemaphoreType.DMA((counts[name],)) for name in COMM + COMM]
        + [pltpu.SemaphoreType.REGULAR((2,))],
        compiler_params=pltpu.CompilerParams(collective_id=0, has_side_effects=True),
        name="whole",
    )(*[operands[name] for name in LOADED])


def on_device(
    latent,
    cond,
    context,
    ctx_cond,
    w_mod,
    norm_gain,
    w_query,
    w_key,
    w_value,
    w_outgate,
    w_decay,
    w_beta,
    decay_rate,
    decay_bias,
    extra_decay,
    out_gain,
    w_out,
):
    operands = {
        "cond": cond,
        "ctx_cond": ctx_cond[None, :],
        "w_mod": w_mod,
        "latent": latent,
        "context": context,
        "gain": norm_gain.reshape(D // HEAD, HEAD),
        "w_key": w_key,
        "w_value": w_value,
        "w_decay": jnp.transpose(w_decay, (1, 2, 0)),
        "w_beta": jnp.transpose(w_beta, (1, 2, 0)),
        "extra": extra_decay,
        "w_query": w_query,
        "w_outgate": w_outgate,
        "out_gain": out_gain[None, :],
        "w_out": w_out,
        "rate": decay_rate,
        "bias": decay_bias,
    }
    sizes = [lax.axis_size(name) for name in (ZAX, XAX, YAX)]
    return whole(operands, *sizes)[None]


def solution(mesh):
    torus = Mesh(
        mesh.devices.reshape(-1, 4, mesh.shape["tp"], mesh.shape["dp"]), (ZAX, XAX, YAX, "dp")
    )
    return jax.shard_map(
        on_device,
        mesh=torus,
        in_specs=(
            P("dp", SP, None),
            P("dp", SP),
            P("dp", SP, None),
            P(SP),
            P(SP, "tp"),
            P(),
            P(None, "tp"),
            P(None, "tp"),
            P(None, "tp"),
            P(None, "tp"),
            P(None, None, "tp"),
            P(None, None, "tp"),
            P(None, "tp"),
            P(None, "tp"),
            P("dp", None, "tp", SP),
            P(),
            P(),
        ),
        out_specs=P("dp", SP_TP, None),
        check_vma=False,
    )
```

```python
import functools

import jax
import jax.numpy as jnp
from jax import lax
from jax.experimental import pallas as pl
from jax.experimental.pallas import tpu as pltpu
from jax.sharding import Mesh
from jax.sharding import PartitionSpec as P

D = 2048
HEAD = 128
BLOCK = 64
HEADS_DEV = 2
CHAINS = 2 * HEADS_DEV
HALF = HEAD // 2
MAP_ROWS = HEAD + HALF + 16
ZAX, XAX, YAX = "sp_0", "sp_1", "tp"
SP = (ZAX, XAX)
SP_TP = (ZAX, XAX, YAX)
MESH = pl.DeviceIdType.MESH
F32 = jnp.float32
BF16 = jnp.bfloat16

norm_eps = 1e-06
beta_scale = 30.0

NN = (((1,), (0,)), ((), ()))
NT = (((1,), (1,)), ((), ()))
TN = (((0,), (0,)), ((), ()))


def dot16(left, right, dims=NN):
    return lax.dot_general(left, right, dims, preferred_element_type=F32)


def mm1(left, right, dims=NN):
    return dot16(left.astype(BF16), right.astype(BF16), dims)


def halves(values):
    high = values.astype(BF16)
    return high, (values - high.astype(F32)).astype(BF16)


def mm3(left, right, dims=NN):
    left_high, left_low = halves(left)
    right_high, right_low = halves(right)
    return dot16(left_high, right_high, dims) + (
        dot16(left_high, right_low, dims) + dot16(left_low, right_high, dims)
    )


def mm_exact_left(left, right, dims=NN):
    high, low = halves(right)
    left = left.astype(BF16)
    return dot16(left, high, dims) + dot16(left, low, dims)


def mm_full(left, right, dims=NN):
    return lax.dot_general(
        left, right, dims, preferred_element_type=F32, precision=lax.Precision.HIGHEST
    )


def silu(values):
    return values * jax.nn.sigmoid(values)


def softplus(values):
    return jnp.maximum(values, 0.0) + jnp.log1p(jnp.exp(-jnp.abs(values)))


def unit_normal(values):
    return values * lax.rsqrt(jnp.sum(values * values, axis=-1, keepdims=True) + norm_eps)


def iota2(shape, dim):
    return lax.broadcasted_iota(jnp.int32, shape, dim)


def unit_inverses(lows, places):
    eye = (iota2((BLOCK, BLOCK), 0) == iota2((BLOCK, BLOCK), 1)).astype(F32)

    def coupling(low, place, level):
        row, col = place
        joined = (row >> (level + 1)) == (col >> (level + 1))
        mask = joined & (((row >> level) & 1) == 1) & (((col >> level) & 1) == 0)
        return jnp.where(mask, low, 0.0)

    results = [eye - coupling(low, place, 0) for low, place in zip(lows, places)]
    for level in range(1, (BLOCK - 1).bit_length()):
        inner = [
            mm1(coupling(low, place, level), result)
            for low, place, result in zip(lows, places, results)
        ]
        results = [result - mm1(result, term) for result, term in zip(results, inner)]
    return results


def chain_terms(keys, values, gram, sums, final, betas, place):
    row, col = place
    eye = iota2((BLOCK, BLOCK), 0) == iota2((BLOCK, BLOCK), 1)
    wide = jnp.broadcast_to(sums, (BLOCK, BLOCK))
    across = jnp.sum(jnp.where(eye, wide, 0.0), axis=0, keepdims=True)
    lower = row >= col
    weights = jnp.where(lower, jnp.exp(jnp.where(lower, wide - across, 0.0)), 0.0)
    low = jnp.where(row > col, gram * betas * weights, 0.0)
    grown = jnp.exp(sums)
    scaled = keys * betas
    right = jnp.concatenate([scaled * grown, values * betas], axis=1)
    decayed = keys * jnp.exp(final - sums)
    return low, right, decayed, weights, grown


def round16(values):
    return values.astype(BF16).astype(F32)


def pack_halves(values):
    return jnp.concatenate([values[: HEAD // 2], values[HEAD // 2 :]], axis=1)


def unpack_halves(values):
    return jnp.concatenate([values[:, : HEAD // 2], values[:, HEAD // 2 :]], axis=0)


def decay_rows(decay):
    high = round16(decay)
    middle = round16(decay - high)
    last = decay - high - middle
    row = iota2((16, HEAD), 0)
    pieces = jnp.where(row == 0, high, jnp.where(row == 1, middle, last))
    return jnp.where(row < 3, pieces, 0.0).astype(BF16)


def put_map(ref, index, decay, near, offset):
    ref[index, :HEAD, :] = near.astype(BF16)
    ref[index, HEAD : HEAD + HALF, :] = pack_halves(offset).astype(BF16)
    ref[index, HEAD + HALF :, :] = decay_rows(decay)


def get_map(ref, index):
    pieces = ref[index, HEAD + HALF :, :].astype(F32)
    decay = pieces[0:1] + pieces[1:2] + pieces[2:3]
    offset = unpack_halves(ref[index, HEAD : HEAD + HALF, :].astype(F32))
    return decay, ref[index, :HEAD, :], offset


def context_steps(ctx_all, rate, bias, direction, h, half):
    nx, nz, rows, _ = ctx_all.shape
    tokens = nx * nz * rows
    data = jnp.concatenate(
        [ctx_all[i, j].astype(F32) for j in range(nz) for i in range(nx)], axis=0
    )
    keys_all = unit_normal(silu(data[:, :HEAD]))
    values_all = silu(
        jnp.where(half == 0, data[:, HEAD : HEAD + HALF], data[:, HEAD + HALF : 2 * HEAD])
    )
    rates = data[:, 2 * HEAD :]
    lane = iota2(rates.shape, 1)
    mine = direction * HEADS_DEV + h
    decay_raw = jnp.sum(jnp.where(lane == mine, rates, 0.0), axis=1, keepdims=True)
    beta_raw = jnp.sum(jnp.where(lane == mine + CHAINS, rates, 0.0), axis=1, keepdims=True)
    log_decay = -rate * softplus(decay_raw + bias)
    betas = jax.nn.sigmoid(beta_raw) * (beta_scale * rate)
    row, col = iota2((BLOCK, BLOCK), 0), iota2((BLOCK, BLOCK), 1)
    flip = direction * (BLOCK - 1)
    sign = 1 - 2 * direction
    place = (flip + sign * row, flip + sign * col)
    tri = (place[0] >= place[1]).astype(F32)
    jobs, lows = [], []
    for b in range(tokens // BLOCK):
        part = slice(b * BLOCK, (b + 1) * BLOCK)
        sums = mm_full(tri, jnp.broadcast_to(log_decay[part], (BLOCK, HEAD)))[:, :1]
        final = jnp.sum(log_decay[part], axis=0, keepdims=True)
        keys, values = keys_all[part], values_all[part]
        gram = mm3(keys, keys, NT)
        low, right, decayed, _, _ = chain_terms(
            keys, values, gram, sums, final, betas[part], place
        )
        lows.append(low)
        jobs.append((right, decayed, final))
    steps = []
    for (right, decayed, final), inverse in zip(jobs, unit_inverses(lows, [place] * len(lows))):
        steps.append((mm1(decayed, mm1(inverse, right), TN), jnp.exp(final)))
    return steps


LOADED = [
    "cond",
    "ctx_cond",
    "w_mod",
    "latent",
    "context",
    "gain",
    "w_key",
    "w_value",
    "w_decay",
    "w_beta",
    "extra",
    "w_query",
    "w_outgate",
    "out_gain",
    "w_out",
    "rate",
    "bias",
]
IN_SMEM = ("rate", "bias")
COMM = ["mod1", "mod2", "ctx", "ctx2", "near", "far", "back", "tp"]


def whole_kernel(nz, nx, ny, hbm, out_ref, loads, load_sem, mem, send, recv, ready):
    z, x, y = lax.axis_index(ZAX), lax.axis_index(XAX), lax.axis_index(YAX)
    span = loads["latent"].shape[1]
    ctx_rows = loads["context"].shape[1]
    blocks = span // BLOCK
    rows_out = span // ny
    inner = HEADS_DEV * HEAD
    low_z = lax.rem(z, 2)
    group = z // 2
    groups = nz // 2
    members = 2 * nx
    own_head, own_half, direction = x // 2, lax.rem(x, 2), low_z
    sign = 1 - 2 * direction

    across = [(dx, dy) for dx in range(nx) for dy in range(ny) if (dx, dy) != (0, 0)]
    across.sort(key=lambda at: -min(at[0], nx - at[0]) - min(at[1], ny - at[1]))
    close = [(dl, dx) for dl in range(2) for dx in range(nx) if (dl, dx) != (0, 0)]
    close.sort(key=lambda at: -at[0] - min(at[1], nx - at[1]))
    along = sorted(range(1, nz), key=lambda dz: -min(dz, nz - dz))

    def across_target(dx, dy):
        return {XAX: lax.rem(x + dx, nx), YAX: lax.rem(y + dy, ny)}

    def close_place(dl, dx):
        return lax.rem(low_z + dl, 2), lax.rem(x + dx, nx)

    barrier = pltpu.get_barrier_semaphore()
    peers = [{ZAX: lax.rem(z + dz, nz)} for dz in range(1, nz)]
    peers += [{XAX: lax.rem(x + dx, nx)} for dx in range(1, nx)]
    peers += [{YAX: lax.rem(y + dy, ny)} for dy in range(1, ny)]
    for target in peers:
        pl.semaphore_signal(barrier, inc=1, device_id=target, device_id_type=MESH)
    fetched = {}
    rate_ref, bias_ref = loads["rate"], loads["bias"]
    for i, name in enumerate(LOADED):
        fetched[name] = pltpu.make_async_copy(hbm[name], loads[name], load_sem.at[i])
        fetched[name].start()

    def remote(kind, k, source, destination, target):
        return pltpu.make_async_remote_copy(
            src_ref=source,
            dst_ref=destination,
            send_sem=send[kind].at[k],
            recv_sem=recv[kind].at[k],
            device_id=target,
            device_id_type=MESH,
        )

    started = []

    def begin(copy):
        copy.start()
        started.append(copy)
        return copy

    def sends_done():
        while started:
            started.pop(0).wait_send()

    part, slots, spread = mem["part"], mem["mod_slots"], mem["spread"]
    width = part.shape[1]
    for name in ("cond", "ctx_cond", "w_mod"):
        fetched[name].wait()
    cond = jnp.concatenate(
        [loads["cond"][...].astype(F32), loads["ctx_cond"][...].astype(F32)], axis=0
    )
    part[...] = dot16(silu(cond).astype(BF16), loads["w_mod"][...])
    pl.semaphore_wait(barrier, len(peers))
    arriving = [
        begin(remote("mod1", dz, part, slots.at[dz], {ZAX: lax.rem(z + dz, nz)})) for dz in along
    ]
    for dx in range(1, nx):
        pl.semaphore_signal(
            ready.at[0], inc=1, device_id={XAX: lax.rem(x + dx, nx)}, device_id_type=MESH
        )
    pl.semaphore_signal(
        ready.at[1],
        inc=1,
        device_id={ZAX: group * 2 + lax.rem(low_z + 1, 2)},
        device_id_type=MESH,
    )
    for name in ("latent", "context", "gain"):
        fetched[name].wait()
    gain = jnp.concatenate(
        [loads["gain"][i : i + 1, :].astype(F32) for i in range(D // HEAD)], axis=1
    )

    def normed(values):
        values = values.astype(F32)
        mean = jnp.mean(values * values, axis=-1, keepdims=True)
        return values * lax.rsqrt(mean + norm_eps) * gain

    mem["normed"][:span, :] = normed(loads["latent"][0])
    mem["normed"][span : span + ctx_rows, :] = normed(loads["context"][0])

    summed = part[...]
    for dz, copy in reversed(list(zip(along, arriving))):
        copy.wait_recv()
        summed = summed + slots[dz]
    spread[y * nx + x] = summed
    pl.semaphore_wait(ready.at[0], nx - 1)
    arriving = [
        begin(
            remote(
                "mod2",
                dy * nx + dx,
                spread.at[y * nx + x],
                spread.at[y * nx + x],
                across_target(dx, dy),
            )
        )
        for dx, dy in across
    ]
    for name in ("w_key", "w_value", "w_decay", "w_beta", "extra", "rate", "bias"):
        fetched[name].wait()
    small = jnp.concatenate(
        [loads[name][d].astype(F32) for name in ("w_decay", "w_beta") for d in range(2)], axis=0
    ).astype(BF16)
    extra = jnp.concatenate([loads["extra"][0, d] for d in range(2)], axis=0)
    eye_span = (iota2((span, span), 0) == iota2((span, span), 1)).astype(F32)
    added = mm_full(eye_span, extra, NT)
    for copy in arriving:
        copy.wait_recv()
    mod = mem["mod"]
    for j in range(ny):
        summed = spread[j * nx]
        for i in range(1, nx):
            summed = summed + spread[j * nx + i]
        mod[:, j * width : (j + 1) * width] = summed

    rows = mem["rows"]
    rows[:span, :] = (
        mem["normed"][:span, :] * (1.0 + mod[0:1, D : 2 * D]) + mod[0:1, :D]
    ).astype(BF16)
    ctx_in = mem["normed"][span : span + ctx_rows, :] * (1.0 + mod[1:2, D : 2 * D]) + mod[1:2, :D]
    rows[span:, :] = jnp.concatenate(
        [ctx_in, jnp.zeros((rows.shape[0] - span - ctx_rows, D), F32)], axis=0
    ).astype(BF16)
    key_raw = round16(dot16(rows[...], loads["w_key"][...]))
    value_raw = round16(dot16(rows[...], loads["w_value"][...]))
    rates_raw = round16(dot16(rows[...], small, NT))

    ctx_z, ctx_all = mem["ctx_z"], mem["ctx_all"]
    ctx_rates = jnp.concatenate(
        [rates_raw[span : span + ctx_rows], jnp.zeros((ctx_rows, HEAD - 2 * CHAINS), F32)], axis=1
    )
    for h in range(HEADS_DEV):
        lanes = slice(h * HEAD, (h + 1) * HEAD)
        ctx_z[h, z] = jnp.concatenate(
            [
                key_raw[span : span + ctx_rows, lanes],
                value_raw[span : span + ctx_rows, lanes],
                ctx_rates,
            ],
            axis=1,
        ).astype(BF16)
    ctx_arriving = [
        begin(
            remote(
                "ctx",
                h * nz + dz,
                ctx_z.at[h, z],
                ctx_z.at[h, z],
                {ZAX: lax.rem(z + dz, nz)},
            )
        )
        for dz in along
        for h in range(HEADS_DEV)
    ]

    lane4 = iota2((1, CHAINS), 1)

    def by_lane(ref):
        line = jnp.zeros((1, CHAINS), F32)
        for d in range(2):
            for h in range(HEADS_DEV):
                line = jnp.where(lane4 == d * HEADS_DEV + h, ref[d, h], line)
        return line

    rate = by_lane(rate_ref)
    log_decay = -rate * softplus(rates_raw[:span, :CHAINS] + by_lane(bias_ref)) + added
    betas = jax.nn.sigmoid(rates_raw[:span, CHAINS:]) * (beta_scale * rate)
    row, col = iota2((BLOCK, BLOCK), 0), iota2((BLOCK, BLOCK), 1)
    places = [(row, col), (BLOCK - 1 - row, BLOCK - 1 - col)]
    tris = [(row >= col).astype(F32), (row <= col).astype(F32)]
    sums = [
        [mm_full(tris[d], log_decay[b * BLOCK : (b + 1) * BLOCK]) for b in range(blocks)]
        for d in range(2)
    ]
    jobs, lows, orders, key_parts = [], [], [], {}
    for h in range(HEADS_DEV):
        lanes = slice(h * HEAD, (h + 1) * HEAD)
        keys_h = unit_normal(silu(key_raw[:span, lanes]))
        values_h = silu(value_raw[:span, lanes])
        for b in range(blocks):
            at = slice(b * BLOCK, (b + 1) * BLOCK)
            keys, values = keys_h[at], values_h[at]
            key_parts[h, b] = keys
            gram = mm3(keys, keys, NT)
            for d in range(2):
                lane = d * HEADS_DEV + h
                cums = sums[d][b][:, lane : lane + 1]
                final = cums[BLOCK - 1 : BLOCK] if d == 0 else cums[0:1]
                low, right, decayed, weights, grown = chain_terms(
                    keys, values, gram, cums, final, betas[at, lane : lane + 1], places[d]
                )
                lows.append(low)
                orders.append(places[d])
                jobs.append((h, d, b, right, decayed, weights, grown, final))
    inverses = unit_inverses(lows, orders)
    found = {}
    for (h, d, b, right, decayed, weights, grown, final), inverse in zip(jobs, inverses):
        solved = mm1(inverse, right)
        step = mm1(decayed, solved, TN)
        found[h, d, b] = (-step[:, :HEAD], step[:, HEAD:], jnp.exp(final), solved, weights, grown)
    maps = mem["maps"]
    before = {}
    for h in range(HEADS_DEV):
        for d in range(2):
            whole = None
            for b in range(blocks) if d == 0 else reversed(range(blocks)):
                near, offset, decay = found[h, d, b][:3]
                before[h, d, b] = whole
                if whole is None:
                    whole = (decay, near, offset)
                else:
                    decay_all, near_all, offset_all = whole
                    moved = mm1(near, jnp.concatenate([near_all, offset_all], axis=1))
                    whole = (
                        decay * decay_all,
                        decay * near_all + decay_all * near + moved[:, :HEAD],
                        decay * offset_all + moved[:, HEAD:] + offset,
                    )
            decay, near, offset = whole
            for c in range(2):
                index = (2 * h + d) * 2 + c
                put_map(maps, index, decay, near, offset[:, c * HALF : (c + 1) * HALF])

    near_slots = mem["near_slots"]

    def map_index(low, at_x):
        return ((at_x // 2) * 2 + low) * 2 + lax.rem(at_x, 2)

    near_slots[0] = maps[map_index(low_z, x)]
    pl.semaphore_wait(ready.at[1], 1)
    arriving = []
    for dl, dx in close:
        low, at_x = close_place(dl, dx)
        arriving.append(
            begin(
                remote(
                    "near",
                    dl * nx + dx,
                    maps.at[map_index(low, at_x)],
                    near_slots.at[dl * nx + dx],
                    {ZAX: group * 2 + low, XAX: at_x},
                )
            )
        )

    for copy in ctx_arriving:
        copy.wait_recv()
    ctx_all[x] = ctx_z[own_head]
    ctx_arriving = []
    for dx in range(1, nx):
        to = lax.rem(x + dx, nx)
        ctx_arriving.append(
            begin(remote("ctx2", dx, ctx_z.at[to // 2], ctx_all.at[x], {XAX: to}))
        )

    for name in ("w_query", "w_outgate", "out_gain"):
        fetched[name].wait()
    query_raw = round16(dot16(rows[:span, :], loads["w_query"][...]))
    mem["gate"][...] = silu(round16(dot16(rows[:span, :], loads["w_outgate"][...])))
    reads, base = mem["reads"], mem["base"]
    for h in range(HEADS_DEV):
        lanes = slice(h * HEAD, (h + 1) * HEAD)
        queries_h = unit_normal(silu(query_raw[:, lanes])) * HEAD ** (-0.5)
        for b in range(blocks):
            at = slice(b * BLOCK, (b + 1) * BLOCK)
            queries = queries_h[at]
            cross = mm1(queries, key_parts[h, b], NT)
            fixed = None
            for d in range(2):
                _, _, _, solved, weights, grown = found[h, d, b]
                read = mm1(cross * weights, solved)
                reader = queries * grown - read[:, :HEAD]
                now = read[:, HEAD:]
                to = slice(d * HEAD, (d + 1) * HEAD)
                if before[h, d, b] is None:
                    reads[h, at, to] = reader.astype(BF16)
                else:
                    decay_all, near_all, offset_all = before[h, d, b]
                    moved = mm1(reader, jnp.concatenate([near_all, offset_all], axis=1))
                    reads[h, at, to] = (decay_all * reader + moved[:, :HEAD]).astype(BF16)
                    now = now + moved[:, HEAD:]
                fixed = now if fixed is None else fixed + now
            base[h, at, :] = fixed

    for copy in arriving:
        copy.wait_recv()
    prefix_near, prefix_offset, prefix_decay = (
        mem["prefix_near"],
        mem["prefix_offset"],
        mem["prefix_decay"],
    )
    def joined(later, earlier, exact):
        decay, near, offset = later
        decay_all, near_all, offset_all = earlier
        both = jnp.concatenate([near_all, offset_all], axis=1)
        moved = mm_exact_left(near, both) if exact else mm3(near, both)
        return (
            decay * decay_all,
            decay * near_all + decay_all * near + moved[:, :HEAD],
            decay[:, :HALF] * offset_all + moved[:, HEAD:] + offset,
        )

    single = []
    for p in range(members):
        source = p + direction * (members - 1 - 2 * p)
        from_low, from_x = source // nx, lax.rem(source, nx)
        slot = lax.rem(low_z - from_low + 2, 2) * nx + lax.rem(x - from_x + nx, nx)
        decay, near, offset = get_map(near_slots, slot)
        single.append((decay, near.astype(F32), offset))
    pairs = [joined(single[p + 1], single[p], True) for p in range(0, members, 2)]
    fours = [joined(pairs[p + 1], pairs[p], False) for p in range(0, members // 2, 2)]
    put_map(mem["sending"], 0, *joined(fours[1], fours[0], False))
    far_slots = mem["far_slots"]

    def far_copy(k):
        return remote(
            "far",
            k,
            mem["sending"].at[0],
            far_slots.at[k],
            {ZAX: lax.rem(z + 2 * k * sign + nz, nz)},
        )

    behind = group + direction * (groups - 1 - 2 * group)
    ahead = groups - 1 - behind
    for k in sorted(range(1, groups), key=lambda k: -min(2 * k, nz - 2 * k)):

        @pl.when(k <= ahead)
        def _(k=k):
            far_copy(k).start()

    third = joined(pairs[2], fours[0], False)
    prefixes = [
        single[0],
        pairs[0],
        joined(single[2], pairs[0], True),
        fours[0],
        joined(single[4], fours[0], True),
        third,
        joined(single[6], third, True),
    ]
    prefix_near[0] = jnp.zeros((HEAD, HEAD), BF16)
    prefix_offset[0] = jnp.zeros((HEAD, HALF), F32)
    prefix_decay[0] = jnp.ones((8, HALF), F32)
    for p, (decay, near, offset) in enumerate(prefixes):
        prefix_near[p + 1] = near.astype(BF16)
        prefix_offset[p + 1] = offset
        prefix_decay[p + 1] = jnp.broadcast_to(decay[:, :HALF], (8, HALF))
    sends_done()
    for copy in ctx_arriving:
        copy.wait_recv()
    steps = context_steps(
        ctx_all, rate_ref[direction, own_head], bias_ref[direction, own_head],
        direction, own_head, own_half,
    )
    ctx_steps, ctx_decay, state = mem["ctx_steps"], mem["ctx_decay"], mem["state"]
    for b, (step, decay) in enumerate(steps):
        ctx_steps[b] = step
        ctx_decay[b] = jnp.broadcast_to(decay, (8, HALF))
    first = direction * (len(steps) - 1)
    now = ctx_steps[first][:, HEAD:]
    for b in range(1, len(steps)):
        at = first + sign * b
        step = ctx_steps[at]
        now = ctx_decay[at, 0:1, :] * now - mm3(step[:, :HEAD], now) + step[:, HEAD:]
    state[...] = now
    for k in reversed(range(1, groups)):

        @pl.when(k <= behind)
        def _(k=k):
            far_copy(k).wait_recv()
            decay, near16, offset = get_map(far_slots, k)
            now = state[...]
            state[...] = decay[:, :HALF] * now + mm_exact_left(near16, now) + offset

    now = state[...]
    now16 = now.astype(BF16)

    def entering(low, at_x):
        place = low * nx + at_x
        p = place + direction * (members - 1 - 2 * place)
        values = prefix_decay[p, 0:1, :] * now + dot16(prefix_near[p], now16) + prefix_offset[p]
        return pack_halves(values).astype(BF16)

    leaving, states = mem["leaving"], mem["states"]
    mine = low_z * nx + x
    spots = [close_place(dl, dx) for dl, dx in close]
    states[mine] = entering(low_z, x)
    for at, values in zip(close, [entering(low, at_x) for low, at_x in spots]):
        leaving[at[0] * nx + at[1]] = values
    arriving = []
    for (dl, dx), (low, at_x) in zip(close, spots):
        k = dl * nx + dx
        arriving.append(
            begin(
                remote(
                    "back", k, leaving.at[k], states.at[mine], {ZAX: group * 2 + low, XAX: at_x}
                )
            )
        )
    for k in range(1, groups):

        @pl.when(k <= ahead)
        def _(k=k):
            far_copy(k).wait_send()

    for copy in arriving:
        copy.wait_recv()

    gated, gathered = mem["gated"], mem["gathered"]
    head_gain = loads["out_gain"][...].astype(F32)
    for h in range(HEADS_DEV):
        whole = jnp.concatenate(
            [
                jnp.concatenate(
                    [unpack_halves(states[d * nx + 2 * h + c].astype(F32)) for c in range(2)],
                    axis=1,
                )
                for d in range(2)
            ],
            axis=0,
        ).astype(BF16)
        total = dot16(reads[h], whole) + base[h]
        scaled = total * lax.rsqrt(jnp.mean(total * total, axis=-1, keepdims=True) + norm_eps)
        lanes = slice(h * HEAD, (h + 1) * HEAD)
        result = (scaled * head_gain * mem["gate"][:, lanes]).astype(BF16)
        for t in range(ny):
            gated[t, :, lanes] = result[t * rows_out : (t + 1) * rows_out]
    arriving = []
    for dy in range(1, ny):
        to = lax.rem(y + dy, ny)
        arriving.append(begin(remote("tp", dy, gated.at[to], gathered.at[dy], {YAX: to})))
    fetched["w_out"].wait()
    w_out = loads["w_out"]

    def product(values, owner):
        return dot16(values, w_out[pl.ds(pl.multiple_of(owner * inner, inner), inner), :])

    mixed = product(gated[y], y)
    for copy in started[:-(ny - 1)]:
        copy.wait_send()
    del started[: -(ny - 1)]
    for dy, copy in zip(range(1, ny), arriving):
        copy.wait_recv()
        mixed = mixed + product(gathered[dy], lax.rem(y - dy + ny, ny))
    own = loads["latent"][0, pl.ds(pl.multiple_of(y * rows_out, 16), rows_out), :].astype(F32)
    out_ref[...] = (own + mod[0:1, 2 * D :] * mixed).astype(BF16)

    sends_done()


def whole(operands, nz, nx, ny):
    span, ctx_rows = operands["latent"].shape[1], operands["context"].shape[1]
    inner = HEADS_DEV * HEAD
    rows_out = span // ny
    width = operands["w_mod"].shape[1]
    members, groups = 2 * nx, nz // 2
    ctx_blocks = nz * nx * ctx_rows // BLOCK
    memory = {
        "part": ((2, width), F32),
        "mod_slots": ((nz, 2, width), F32),
        "spread": ((nx * ny, 2, width), F32),
        "mod": ((2, width * ny), F32),
        "normed": ((span + ctx_rows, D), F32),
        "rows": ((span + 16, D), BF16),
        "ctx_z": ((HEADS_DEV, nz, ctx_rows, 3 * HEAD), BF16),
        "ctx_all": ((nx, nz, ctx_rows, 3 * HEAD), BF16),
        "maps": ((2 * CHAINS, MAP_ROWS, HEAD), BF16),
        "near_slots": ((members, MAP_ROWS, HEAD), BF16),
        "gate": ((span, inner), F32),
        "reads": ((HEADS_DEV, span, 2 * HEAD), BF16),
        "base": ((HEADS_DEV, span, HEAD), F32),
        "prefix_near": ((members, HEAD, HEAD), BF16),
        "prefix_offset": ((members, HEAD, HALF), F32),
        "prefix_decay": ((members, 8, HALF), F32),
        "sending": ((1, MAP_ROWS, HEAD), BF16),
        "far_slots": ((groups, MAP_ROWS, HEAD), BF16),
        "ctx_steps": ((ctx_blocks, HEAD, HEAD + HALF), F32),
        "ctx_decay": ((ctx_blocks, 8, HALF), F32),
        "state": ((HEAD, HALF), F32),
        "leaving": ((members, HALF, HEAD), BF16),
        "states": ((members, HALF, HEAD), BF16),
        "gated": ((ny, rows_out, inner), BF16),
        "gathered": ((ny, rows_out, inner), BF16),
    }
    counts = {
        "mod1": nz,
        "mod2": nx * ny,
        "ctx": HEADS_DEV * nz,
        "ctx2": nx,
        "near": members,
        "far": groups,
        "back": members,
        "tp": ny,
    }

    def kernel(*refs):
        refs = list(refs)

        def take(names):
            return {name: refs.pop(0) for name in names}

        hbm = take(LOADED)
        out_ref = refs.pop(0)
        loads = take(LOADED)
        load_sem = refs.pop(0)
        mem = take(memory)
        send, recv = take(COMM), take(COMM)
        whole_kernel(
            nz, nx, ny, hbm, out_ref, loads, load_sem, mem, send, recv, refs.pop(0)
        )

    return pl.pallas_call(
        kernel,
        out_shape=pltpu.VMEM((rows_out, D), BF16),
        in_specs=[pl.BlockSpec(memory_space=pl.ANY)] * len(LOADED),
        out_specs=pl.BlockSpec(memory_space=pltpu.VMEM),
        scratch_shapes=[
            (pltpu.SMEM if n in IN_SMEM else pltpu.VMEM)(operands[n].shape, operands[n].dtype)
            for n in LOADED
        ]
        + [pltpu.SemaphoreType.DMA((len(LOADED),))]
        + [pltpu.VMEM(*memory[name]) for name in memory]
        + [pltpu.SemaphoreType.DMA((counts[name],)) for name in COMM + COMM]
        + [pltpu.SemaphoreType.REGULAR((2,))],
        compiler_params=pltpu.CompilerParams(collective_id=0, has_side_effects=True),
        name="whole",
    )(*[operands[name] for name in LOADED])


def on_device(
    latent,
    cond,
    context,
    ctx_cond,
    w_mod,
    norm_gain,
    w_query,
    w_key,
    w_value,
    w_outgate,
    w_decay,
    w_beta,
    decay_rate,
    decay_bias,
    extra_decay,
    out_gain,
    w_out,
):
    operands = {
        "cond": cond,
        "ctx_cond": ctx_cond[None, :],
        "w_mod": w_mod,
        "latent": latent,
        "context": context,
        "gain": norm_gain.reshape(D // HEAD, HEAD),
        "w_key": w_key,
        "w_value": w_value,
        "w_decay": jnp.transpose(w_decay, (1, 2, 0)),
        "w_beta": jnp.transpose(w_beta, (1, 2, 0)),
        "extra": extra_decay,
        "w_query": w_query,
        "w_outgate": w_outgate,
        "out_gain": out_gain[None, :],
        "w_out": w_out,
        "rate": decay_rate,
        "bias": decay_bias,
    }
    sizes = [lax.axis_size(name) for name in (ZAX, XAX, YAX)]
    return whole(operands, *sizes)[None]


def solution(mesh):
    torus = Mesh(
        mesh.devices.reshape(-1, 4, mesh.shape["tp"], mesh.shape["dp"]), (ZAX, XAX, YAX, "dp")
    )
    return jax.shard_map(
        on_device,
        mesh=torus,
        in_specs=(
            P("dp", SP, None),
            P("dp", SP),
            P("dp", SP, None),
            P(SP),
            P(SP, "tp"),
            P(),
            P(None, "tp"),
            P(None, "tp"),
            P(None, "tp"),
            P(None, "tp"),
            P(None, None, "tp"),
            P(None, None, "tp"),
            P(None, "tp"),
            P(None, "tp"),
            P("dp", None, "tp", SP),
            P(),
            P(),
        ),
        out_specs=P("dp", SP_TP, None),
        check_vma=False,
    )
```

```python
import functools

import jax
import jax.numpy as jnp
from jax import lax
from jax.experimental import pallas as pl
from jax.experimental.pallas import tpu as pltpu
from jax.sharding import Mesh
from jax.sharding import PartitionSpec as P

D = 2048
HEAD = 128
BLOCK = 64
HEADS_DEV = 2
CHAINS = 2 * HEADS_DEV
HALF = HEAD // 2
MAP_ROWS = HEAD + HALF + 16
ZAX, XAX, YAX = "sp_0", "sp_1", "tp"
SP = (ZAX, XAX)
SP_TP = (ZAX, XAX, YAX)
MESH = pl.DeviceIdType.MESH
F32 = jnp.float32
BF16 = jnp.bfloat16

norm_eps = 1e-06
beta_scale = 30.0

NN = (((1,), (0,)), ((), ()))
NT = (((1,), (1,)), ((), ()))
TN = (((0,), (0,)), ((), ()))


def dot16(left, right, dims=NN):
    return lax.dot_general(left, right, dims, preferred_element_type=F32)


def mm1(left, right, dims=NN):
    return dot16(left.astype(BF16), right.astype(BF16), dims)


def halves(values):
    high = values.astype(BF16)
    return high, (values - high.astype(F32)).astype(BF16)


def mm_exact_left(left, right, dims=NN):
    high, low = halves(right)
    left = left.astype(BF16)
    return dot16(left, high, dims) + dot16(left, low, dims)


def silu(values):
    return values * jax.nn.sigmoid(values)


def softplus(values):
    return jnp.maximum(values, 0.0) + jnp.log1p(jnp.exp(-jnp.abs(values)))


def unit_normal(values):
    return values * lax.rsqrt(jnp.sum(values * values, axis=-1, keepdims=True) + norm_eps)


def iota2(shape, dim):
    return lax.broadcasted_iota(jnp.int32, shape, dim)


def unit_inverses(lows, places):
    eye = (iota2((BLOCK, BLOCK), 0) == iota2((BLOCK, BLOCK), 1)).astype(F32)

    def coupling(low, place, level):
        row, col = place
        joined = (row >> (level + 1)) == (col >> (level + 1))
        mask = joined & (((row >> level) & 1) == 1) & (((col >> level) & 1) == 0)
        return jnp.where(mask, low, 0.0)

    results = [eye - coupling(low, place, 0) for low, place in zip(lows, places)]
    for level in range(1, (BLOCK - 1).bit_length()):
        inner = [
            mm1(coupling(low, place, level), result)
            for low, place, result in zip(lows, places, results)
        ]
        results = [result - mm1(result, term) for result, term in zip(results, inner)]
    return results


def chain_terms(keys, values, gram, sums, final, betas, place):
    row, col = place
    eye = iota2((BLOCK, BLOCK), 0) == iota2((BLOCK, BLOCK), 1)
    wide = jnp.broadcast_to(sums, (BLOCK, BLOCK))
    across = jnp.sum(jnp.where(eye, wide, 0.0), axis=0, keepdims=True)
    lower = row >= col
    weights = jnp.where(lower, jnp.exp(jnp.where(lower, wide - across, 0.0)), 0.0)
    low = jnp.where(row > col, gram * betas * weights, 0.0)
    grown = jnp.exp(sums)
    scaled = keys * betas
    right = jnp.concatenate([scaled * grown, values * betas], axis=1)
    decayed = keys * jnp.exp(final - sums)
    return low, right, decayed, weights, grown


def round16(values):
    return values.astype(BF16).astype(F32)


def pack_halves(values):
    return jnp.concatenate([values[: HEAD // 2], values[HEAD // 2 :]], axis=1)


def unpack_halves(values):
    return jnp.concatenate([values[:, : HEAD // 2], values[:, HEAD // 2 :]], axis=0)


def decay_rows(decay):
    high = round16(decay)
    middle = round16(decay - high)
    last = decay - high - middle
    row = iota2((16, HEAD), 0)
    pieces = jnp.where(row == 0, high, jnp.where(row == 1, middle, last))
    return jnp.where(row < 3, pieces, 0.0).astype(BF16)


def put_map(ref, index, decay, near, offset):
    ref[index, :HEAD, :] = near.astype(BF16)
    ref[index, HEAD : HEAD + HALF, :] = pack_halves(offset).astype(BF16)
    ref[index, HEAD + HALF :, :] = decay_rows(decay)


def get_map(ref, index):
    pieces = ref[index, HEAD + HALF :, :].astype(F32)
    decay = pieces[0:1] + pieces[1:2] + pieces[2:3]
    offset = unpack_halves(ref[index, HEAD : HEAD + HALF, :].astype(F32))
    return decay, ref[index, :HEAD, :], offset


def context_steps(ctx_all, rate, bias, direction, h, half):
    nx, nz, rows, _ = ctx_all.shape
    tokens = nx * nz * rows
    data = jnp.concatenate(
        [ctx_all[i, j].astype(F32) for j in range(nz) for i in range(nx)], axis=0
    )
    keys_all = unit_normal(silu(data[:, :HEAD]))
    values_all = silu(
        jnp.where(half == 0, data[:, HEAD : HEAD + HALF], data[:, HEAD + HALF : 2 * HEAD])
    )
    rates = data[:, 2 * HEAD :]
    lane = iota2(rates.shape, 1)
    mine = direction * HEADS_DEV + h
    decay_raw = jnp.sum(jnp.where(lane == mine, rates, 0.0), axis=1, keepdims=True)
    beta_raw = jnp.sum(jnp.where(lane == mine + CHAINS, rates, 0.0), axis=1, keepdims=True)
    log_decay = -rate * softplus(decay_raw + bias)
    betas = jax.nn.sigmoid(beta_raw) * (beta_scale * rate)
    row, col = iota2((BLOCK, BLOCK), 0), iota2((BLOCK, BLOCK), 1)
    flip = direction * (BLOCK - 1)
    sign = 1 - 2 * direction
    place = (flip + sign * row, flip + sign * col)
    tri = (place[0] >= place[1]).astype(F32)
    jobs, lows = [], []
    for b in range(tokens // BLOCK):
        part = slice(b * BLOCK, (b + 1) * BLOCK)
        sums = mm_exact_left(tri, jnp.broadcast_to(log_decay[part], (BLOCK, HEAD)))[:, :1]
        final = jnp.sum(log_decay[part], axis=0, keepdims=True)
        keys, values = keys_all[part], values_all[part]
        gram = mm1(keys, keys, NT)
        low, right, decayed, _, _ = chain_terms(
            keys, values, gram, sums, final, betas[part], place
        )
        lows.append(low)
        jobs.append((right, decayed, final))
    steps = []
    for (right, decayed, final), inverse in zip(jobs, unit_inverses(lows, [place] * len(lows))):
        steps.append((mm1(decayed, mm1(inverse, right), TN), jnp.exp(final)))
    return steps


LOADED = [
    "cond",
    "ctx_cond",
    "w_mod",
    "latent",
    "context",
    "gain",
    "w_key",
    "w_value",
    "w_decay",
    "w_beta",
    "extra",
    "w_query",
    "w_outgate",
    "out_gain",
    "w_out",
    "rate",
    "bias",
]
IN_SMEM = ("rate", "bias")
COMM = ["mod1", "mod2", "ctx", "ctx2", "near", "far", "back", "tp"]


def whole_kernel(nz, nx, ny, hbm, out_ref, loads, load_sem, mem, send, recv, ready):
    z, x, y = lax.axis_index(ZAX), lax.axis_index(XAX), lax.axis_index(YAX)
    span = loads["latent"].shape[1]
    ctx_rows = loads["context"].shape[1]
    blocks = span // BLOCK
    rows_out = span // ny
    inner = HEADS_DEV * HEAD
    low_z = lax.rem(z, 2)
    group = z // 2
    groups = nz // 2
    members = 2 * nx
    own_head, own_half, direction = x // 2, lax.rem(x, 2), low_z
    sign = 1 - 2 * direction

    across = [(dx, dy) for dx in range(nx) for dy in range(ny) if (dx, dy) != (0, 0)]
    across.sort(key=lambda at: -min(at[0], nx - at[0]) - min(at[1], ny - at[1]))
    close = [(dl, dx) for dl in range(2) for dx in range(nx) if (dl, dx) != (0, 0)]
    close.sort(key=lambda at: -at[0] - min(at[1], nx - at[1]))
    along = sorted(range(1, nz), key=lambda dz: -min(dz, nz - dz))

    def across_target(dx, dy):
        return {XAX: lax.rem(x + dx, nx), YAX: lax.rem(y + dy, ny)}

    def close_place(dl, dx):
        return lax.rem(low_z + dl, 2), lax.rem(x + dx, nx)

    barrier = pltpu.get_barrier_semaphore()
    peers = [{ZAX: lax.rem(z + dz, nz)} for dz in range(1, nz)]
    peers += [{XAX: lax.rem(x + dx, nx)} for dx in range(1, nx)]
    peers += [{YAX: lax.rem(y + dy, ny)} for dy in range(1, ny)]
    for target in peers:
        pl.semaphore_signal(barrier, inc=1, device_id=target, device_id_type=MESH)
    fetched = {}
    rate_ref, bias_ref = loads["rate"], loads["bias"]
    for i, name in enumerate(LOADED):
        fetched[name] = pltpu.make_async_copy(hbm[name], loads[name], load_sem.at[i])
        fetched[name].start()

    def remote(kind, k, source, destination, target):
        return pltpu.make_async_remote_copy(
            src_ref=source,
            dst_ref=destination,
            send_sem=send[kind].at[k],
            recv_sem=recv[kind].at[k],
            device_id=target,
            device_id_type=MESH,
        )

    started = []

    def begin(copy):
        copy.start()
        started.append(copy)
        return copy

    def sends_done():
        while started:
            started.pop(0).wait_send()

    part, slots, spread = mem["part"], mem["mod_slots"], mem["spread"]
    width = part.shape[1]
    for name in ("cond", "ctx_cond", "w_mod"):
        fetched[name].wait()
    cond = jnp.concatenate(
        [loads["cond"][...].astype(F32), loads["ctx_cond"][...].astype(F32)], axis=0
    )
    part[...] = dot16(silu(cond).astype(BF16), loads["w_mod"][...])
    pl.semaphore_wait(barrier, len(peers))
    arriving = [
        begin(remote("mod1", dz, part, slots.at[dz], {ZAX: lax.rem(z + dz, nz)})) for dz in along
    ]
    for dx in range(1, nx):
        pl.semaphore_signal(
            ready.at[0], inc=1, device_id={XAX: lax.rem(x + dx, nx)}, device_id_type=MESH
        )
    pl.semaphore_signal(
        ready.at[1],
        inc=1,
        device_id={ZAX: group * 2 + lax.rem(low_z + 1, 2)},
        device_id_type=MESH,
    )
    for name in ("latent", "context", "gain"):
        fetched[name].wait()
    gain = jnp.concatenate(
        [loads["gain"][i : i + 1, :].astype(F32) for i in range(D // HEAD)], axis=1
    )

    def normed(values):
        values = values.astype(F32)
        mean = jnp.mean(values * values, axis=-1, keepdims=True)
        return values * lax.rsqrt(mean + norm_eps) * gain

    mem["normed"][:span, :] = normed(loads["latent"][0])
    mem["normed"][span : span + ctx_rows, :] = normed(loads["context"][0])

    summed = part[...]
    for dz, copy in reversed(list(zip(along, arriving))):
        copy.wait_recv()
        summed = summed + slots[dz]
    spread[y * nx + x] = summed
    pl.semaphore_wait(ready.at[0], nx - 1)
    arriving = [
        begin(
            remote(
                "mod2",
                dy * nx + dx,
                spread.at[y * nx + x],
                spread.at[y * nx + x],
                across_target(dx, dy),
            )
        )
        for dx, dy in across
    ]
    for name in ("w_key", "w_value", "w_decay", "w_beta", "extra", "rate", "bias"):
        fetched[name].wait()
    small = jnp.concatenate(
        [loads[name][d].astype(F32) for name in ("w_decay", "w_beta") for d in range(2)], axis=0
    ).astype(BF16)
    extra = jnp.concatenate([loads["extra"][0, d] for d in range(2)], axis=0)
    eye_span = (iota2((span, span), 0) == iota2((span, span), 1)).astype(F32)
    added = mm_exact_left(eye_span, extra, NT)
    for copy in arriving:
        copy.wait_recv()
    mod = mem["mod"]
    for j in range(ny):
        summed = spread[j * nx]
        for i in range(1, nx):
            summed = summed + spread[j * nx + i]
        mod[:, j * width : (j + 1) * width] = summed

    rows = mem["rows"]
    rows[:span, :] = (
        mem["normed"][:span, :] * (1.0 + mod[0:1, D : 2 * D]) + mod[0:1, :D]
    ).astype(BF16)
    ctx_in = mem["normed"][span : span + ctx_rows, :] * (1.0 + mod[1:2, D : 2 * D]) + mod[1:2, :D]
    rows[span:, :] = jnp.concatenate(
        [ctx_in, jnp.zeros((rows.shape[0] - span - ctx_rows, D), F32)], axis=0
    ).astype(BF16)
    key_raw = round16(dot16(rows[...], loads["w_key"][...]))
    value_raw = round16(dot16(rows[...], loads["w_value"][...]))
    rates_raw = round16(dot16(rows[...], small, NT))

    ctx_z, ctx_all = mem["ctx_z"], mem["ctx_all"]
    ctx_rates = jnp.concatenate(
        [rates_raw[span : span + ctx_rows], jnp.zeros((ctx_rows, HEAD - 2 * CHAINS), F32)], axis=1
    )
    for h in range(HEADS_DEV):
        lanes = slice(h * HEAD, (h + 1) * HEAD)
        ctx_z[h, z] = jnp.concatenate(
            [
                key_raw[span : span + ctx_rows, lanes],
                value_raw[span : span + ctx_rows, lanes],
                ctx_rates,
            ],
            axis=1,
        ).astype(BF16)
    ctx_arriving = [
        begin(
            remote(
                "ctx",
                h * nz + dz,
                ctx_z.at[h, z],
                ctx_z.at[h, z],
                {ZAX: lax.rem(z + dz, nz)},
            )
        )
        for dz in along
        for h in range(HEADS_DEV)
    ]

    lane4 = iota2((1, CHAINS), 1)

    def by_lane(ref):
        line = jnp.zeros((1, CHAINS), F32)
        for d in range(2):
            for h in range(HEADS_DEV):
                line = jnp.where(lane4 == d * HEADS_DEV + h, ref[d, h], line)
        return line

    rate = by_lane(rate_ref)
    log_decay = -rate * softplus(rates_raw[:span, :CHAINS] + by_lane(bias_ref)) + added
    betas = jax.nn.sigmoid(rates_raw[:span, CHAINS:]) * (beta_scale * rate)
    row, col = iota2((BLOCK, BLOCK), 0), iota2((BLOCK, BLOCK), 1)
    places = [(row, col), (BLOCK - 1 - row, BLOCK - 1 - col)]
    tris = [(row >= col).astype(F32), (row <= col).astype(F32)]
    sums = [
        [
            mm_exact_left(tris[d], log_decay[b * BLOCK : (b + 1) * BLOCK])
            for b in range(blocks)
        ]
        for d in range(2)
    ]
    jobs, lows, orders, key_parts = [], [], [], {}
    for h in range(HEADS_DEV):
        lanes = slice(h * HEAD, (h + 1) * HEAD)
        keys_h = unit_normal(silu(key_raw[:span, lanes]))
        values_h = silu(value_raw[:span, lanes])
        for b in range(blocks):
            at = slice(b * BLOCK, (b + 1) * BLOCK)
            keys, values = keys_h[at], values_h[at]
            key_parts[h, b] = keys
            gram = mm1(keys, keys, NT)
            for d in range(2):
                lane = d * HEADS_DEV + h
                cums = sums[d][b][:, lane : lane + 1]
                final = cums[BLOCK - 1 : BLOCK] if d == 0 else cums[0:1]
                low, right, decayed, weights, grown = chain_terms(
                    keys, values, gram, cums, final, betas[at, lane : lane + 1], places[d]
                )
                lows.append(low)
                orders.append(places[d])
                jobs.append((h, d, b, right, decayed, weights, grown, final))
    inverses = unit_inverses(lows, orders)
    found = {}
    for (h, d, b, right, decayed, weights, grown, final), inverse in zip(jobs, inverses):
        solved = mm1(inverse, right)
        step = mm1(decayed, solved, TN)
        found[h, d, b] = (-step[:, :HEAD], step[:, HEAD:], jnp.exp(final), solved, weights, grown)
    maps = mem["maps"]
    before = {}
    for h in range(HEADS_DEV):
        for d in range(2):
            whole = None
            for b in range(blocks) if d == 0 else reversed(range(blocks)):
                near, offset, decay = found[h, d, b][:3]
                before[h, d, b] = whole
                if whole is None:
                    whole = (decay, near, offset)
                else:
                    decay_all, near_all, offset_all = whole
                    moved = mm1(near, jnp.concatenate([near_all, offset_all], axis=1))
                    whole = (
                        decay * decay_all,
                        decay * near_all + decay_all * near + moved[:, :HEAD],
                        decay * offset_all + moved[:, HEAD:] + offset,
                    )
            decay, near, offset = whole
            for c in range(2):
                index = (2 * h + d) * 2 + c
                put_map(maps, index, decay, near, offset[:, c * HALF : (c + 1) * HALF])

    near_slots = mem["near_slots"]

    def map_index(low, at_x):
        return ((at_x // 2) * 2 + low) * 2 + lax.rem(at_x, 2)

    near_slots[0] = maps[map_index(low_z, x)]
    pl.semaphore_wait(ready.at[1], 1)
    arriving = []
    for dl, dx in close:
        low, at_x = close_place(dl, dx)
        arriving.append(
            begin(
                remote(
                    "near",
                    dl * nx + dx,
                    maps.at[map_index(low, at_x)],
                    near_slots.at[dl * nx + dx],
                    {ZAX: group * 2 + low, XAX: at_x},
                )
            )
        )

    for copy in ctx_arriving:
        copy.wait_recv()
    ctx_all[x] = ctx_z[own_head]
    ctx_arriving = []
    for dx in range(1, nx):
        to = lax.rem(x + dx, nx)
        ctx_arriving.append(
            begin(remote("ctx2", dx, ctx_z.at[to // 2], ctx_all.at[x], {XAX: to}))
        )

    for name in ("w_query", "w_outgate", "out_gain"):
        fetched[name].wait()
    query_raw = round16(dot16(rows[:span, :], loads["w_query"][...]))
    mem["gate"][...] = silu(round16(dot16(rows[:span, :], loads["w_outgate"][...])))
    reads, base = mem["reads"], mem["base"]
    for h in range(HEADS_DEV):
        lanes = slice(h * HEAD, (h + 1) * HEAD)
        queries_h = unit_normal(silu(query_raw[:, lanes])) * HEAD ** (-0.5)
        for b in range(blocks):
            at = slice(b * BLOCK, (b + 1) * BLOCK)
            queries = queries_h[at]
            cross = mm1(queries, key_parts[h, b], NT)
            fixed = None
            for d in range(2):
                _, _, _, solved, weights, grown = found[h, d, b]
                read = mm1(cross * weights, solved)
                reader = queries * grown - read[:, :HEAD]
                now = read[:, HEAD:]
                to = slice(d * HEAD, (d + 1) * HEAD)
                if before[h, d, b] is None:
                    reads[h, at, to] = reader.astype(BF16)
                else:
                    decay_all, near_all, offset_all = before[h, d, b]
                    moved = mm1(reader, jnp.concatenate([near_all, offset_all], axis=1))
                    reads[h, at, to] = (decay_all * reader + moved[:, :HEAD]).astype(BF16)
                    now = now + moved[:, HEAD:]
                fixed = now if fixed is None else fixed + now
            base[h, at, :] = fixed

    for copy in arriving:
        copy.wait_recv()
    prefix_near, prefix_offset, prefix_decay = (
        mem["prefix_near"],
        mem["prefix_offset"],
        mem["prefix_decay"],
    )
    def joined(later, earlier):
        decay, near, offset = later
        decay_all, near_all, offset_all = earlier
        both = jnp.concatenate([near_all, offset_all], axis=1)
        moved = mm1(near, both)
        return (
            decay * decay_all,
            decay * near_all + decay_all * near + moved[:, :HEAD],
            decay[:, :HALF] * offset_all + moved[:, HEAD:] + offset,
        )

    single = []
    for p in range(members):
        source = p + direction * (members - 1 - 2 * p)
        from_low, from_x = source // nx, lax.rem(source, nx)
        slot = lax.rem(low_z - from_low + 2, 2) * nx + lax.rem(x - from_x + nx, nx)
        decay, near, offset = get_map(near_slots, slot)
        single.append((decay, near.astype(F32), offset))
    pairs = [joined(single[p + 1], single[p]) for p in range(0, members, 2)]
    fours = [joined(pairs[p + 1], pairs[p]) for p in range(0, members // 2, 2)]
    put_map(mem["sending"], 0, *joined(fours[1], fours[0]))
    far_slots = mem["far_slots"]

    def far_copy(k):
        return remote(
            "far",
            k,
            mem["sending"].at[0],
            far_slots.at[k],
            {ZAX: lax.rem(z + 2 * k * sign + nz, nz)},
        )

    behind = group + direction * (groups - 1 - 2 * group)
    ahead = groups - 1 - behind
    for k in sorted(range(1, groups), key=lambda k: -min(2 * k, nz - 2 * k)):

        @pl.when(k <= ahead)
        def _(k=k):
            far_copy(k).start()

    third = joined(pairs[2], fours[0])
    prefixes = [
        single[0],
        pairs[0],
        joined(single[2], pairs[0]),
        fours[0],
        joined(single[4], fours[0]),
        third,
        joined(single[6], third),
    ]
    prefix_near[0] = jnp.zeros((HEAD, HEAD), BF16)
    prefix_offset[0] = jnp.zeros((HEAD, HALF), F32)
    prefix_decay[0] = jnp.ones((8, HALF), F32)
    for p, (decay, near, offset) in enumerate(prefixes):
        prefix_near[p + 1] = near.astype(BF16)
        prefix_offset[p + 1] = offset
        prefix_decay[p + 1] = jnp.broadcast_to(decay[:, :HALF], (8, HALF))
    sends_done()
    for copy in ctx_arriving:
        copy.wait_recv()
    steps = context_steps(
        ctx_all, rate_ref[direction, own_head], bias_ref[direction, own_head],
        direction, own_head, own_half,
    )
    ctx_steps, ctx_decay, state = mem["ctx_steps"], mem["ctx_decay"], mem["state"]
    for b, (step, decay) in enumerate(steps):
        ctx_steps[b] = step
        ctx_decay[b] = jnp.broadcast_to(decay, (8, HALF))
    first = direction * (len(steps) - 1)
    now = ctx_steps[first][:, HEAD:]
    for b in range(1, len(steps)):
        at = first + sign * b
        step = ctx_steps[at]
        now = ctx_decay[at, 0:1, :] * now - mm1(step[:, :HEAD], now) + step[:, HEAD:]
    state[...] = now
    for k in reversed(range(1, groups)):

        @pl.when(k <= behind)
        def _(k=k):
            far_copy(k).wait_recv()
            decay, near16, offset = get_map(far_slots, k)
            now = state[...]
            state[...] = decay[:, :HALF] * now + mm1(near16, now) + offset

    now = state[...]
    now16 = now.astype(BF16)

    def entering(low, at_x):
        place = low * nx + at_x
        p = place + direction * (members - 1 - 2 * place)
        values = prefix_decay[p, 0:1, :] * now + dot16(prefix_near[p], now16) + prefix_offset[p]
        return pack_halves(values).astype(BF16)

    leaving, states = mem["leaving"], mem["states"]
    mine = low_z * nx + x
    spots = [close_place(dl, dx) for dl, dx in close]
    states[mine] = entering(low_z, x)
    for at, values in zip(close, [entering(low, at_x) for low, at_x in spots]):
        leaving[at[0] * nx + at[1]] = values
    arriving = []
    for (dl, dx), (low, at_x) in zip(close, spots):
        k = dl * nx + dx
        arriving.append(
            begin(
                remote(
                    "back", k, leaving.at[k], states.at[mine], {ZAX: group * 2 + low, XAX: at_x}
                )
            )
        )
    for k in range(1, groups):

        @pl.when(k <= ahead)
        def _(k=k):
            far_copy(k).wait_send()

    for copy in arriving:
        copy.wait_recv()

    gated, gathered = mem["gated"], mem["gathered"]
    head_gain = loads["out_gain"][...].astype(F32)
    for h in range(HEADS_DEV):
        whole = jnp.concatenate(
            [
                jnp.concatenate(
                    [unpack_halves(states[d * nx + 2 * h + c].astype(F32)) for c in range(2)],
                    axis=1,
                )
                for d in range(2)
            ],
            axis=0,
        ).astype(BF16)
        total = dot16(reads[h], whole) + base[h]
        scaled = total * lax.rsqrt(jnp.mean(total * total, axis=-1, keepdims=True) + norm_eps)
        lanes = slice(h * HEAD, (h + 1) * HEAD)
        result = (scaled * head_gain * mem["gate"][:, lanes]).astype(BF16)
        for t in range(ny):
            gated[t, :, lanes] = result[t * rows_out : (t + 1) * rows_out]
    arriving = []
    for dy in range(1, ny):
        to = lax.rem(y + dy, ny)
        arriving.append(begin(remote("tp", dy, gated.at[to], gathered.at[dy], {YAX: to})))
    fetched["w_out"].wait()
    w_out = loads["w_out"]

    def product(values, owner):
        return dot16(values, w_out[pl.ds(pl.multiple_of(owner * inner, inner), inner), :])

    mixed = product(gated[y], y)
    for copy in started[:-(ny - 1)]:
        copy.wait_send()
    del started[: -(ny - 1)]
    for dy, copy in zip(range(1, ny), arriving):
        copy.wait_recv()
        mixed = mixed + product(gathered[dy], lax.rem(y - dy + ny, ny))
    own = loads["latent"][0, pl.ds(pl.multiple_of(y * rows_out, 16), rows_out), :].astype(F32)
    out_ref[...] = (own + mod[0:1, 2 * D :] * mixed).astype(BF16)

    sends_done()


def whole(operands, nz, nx, ny):
    span, ctx_rows = operands["latent"].shape[1], operands["context"].shape[1]
    inner = HEADS_DEV * HEAD
    rows_out = span // ny
    width = operands["w_mod"].shape[1]
    members, groups = 2 * nx, nz // 2
    ctx_blocks = nz * nx * ctx_rows // BLOCK
    memory = {
        "part": ((2, width), F32),
        "mod_slots": ((nz, 2, width), F32),
        "spread": ((nx * ny, 2, width), F32),
        "mod": ((2, width * ny), F32),
        "normed": ((span + ctx_rows, D), F32),
        "rows": ((span + 16, D), BF16),
        "ctx_z": ((HEADS_DEV, nz, ctx_rows, 3 * HEAD), BF16),
        "ctx_all": ((nx, nz, ctx_rows, 3 * HEAD), BF16),
        "maps": ((2 * CHAINS, MAP_ROWS, HEAD), BF16),
        "near_slots": ((members, MAP_ROWS, HEAD), BF16),
        "gate": ((span, inner), F32),
        "reads": ((HEADS_DEV, span, 2 * HEAD), BF16),
        "base": ((HEADS_DEV, span, HEAD), F32),
        "prefix_near": ((members, HEAD, HEAD), BF16),
        "prefix_offset": ((members, HEAD, HALF), F32),
        "prefix_decay": ((members, 8, HALF), F32),
        "sending": ((1, MAP_ROWS, HEAD), BF16),
        "far_slots": ((groups, MAP_ROWS, HEAD), BF16),
        "ctx_steps": ((ctx_blocks, HEAD, HEAD + HALF), F32),
        "ctx_decay": ((ctx_blocks, 8, HALF), F32),
        "state": ((HEAD, HALF), F32),
        "leaving": ((members, HALF, HEAD), BF16),
        "states": ((members, HALF, HEAD), BF16),
        "gated": ((ny, rows_out, inner), BF16),
        "gathered": ((ny, rows_out, inner), BF16),
    }
    counts = {
        "mod1": nz,
        "mod2": nx * ny,
        "ctx": HEADS_DEV * nz,
        "ctx2": nx,
        "near": members,
        "far": groups,
        "back": members,
        "tp": ny,
    }

    def kernel(*refs):
        refs = list(refs)

        def take(names):
            return {name: refs.pop(0) for name in names}

        hbm = take(LOADED)
        out_ref = refs.pop(0)
        loads = take(LOADED)
        load_sem = refs.pop(0)
        mem = take(memory)
        send, recv = take(COMM), take(COMM)
        whole_kernel(
            nz, nx, ny, hbm, out_ref, loads, load_sem, mem, send, recv, refs.pop(0)
        )

    return pl.pallas_call(
        kernel,
        out_shape=pltpu.VMEM((rows_out, D), BF16),
        in_specs=[pl.BlockSpec(memory_space=pl.ANY)] * len(LOADED),
        out_specs=pl.BlockSpec(memory_space=pltpu.VMEM),
        scratch_shapes=[
            (pltpu.SMEM if n in IN_SMEM else pltpu.VMEM)(operands[n].shape, operands[n].dtype)
            for n in LOADED
        ]
        + [pltpu.SemaphoreType.DMA((len(LOADED),))]
        + [pltpu.VMEM(*memory[name]) for name in memory]
        + [pltpu.SemaphoreType.DMA((counts[name],)) for name in COMM + COMM]
        + [pltpu.SemaphoreType.REGULAR((2,))],
        compiler_params=pltpu.CompilerParams(collective_id=0, has_side_effects=True),
        name="whole",
    )(*[operands[name] for name in LOADED])


def on_device(
    latent,
    cond,
    context,
    ctx_cond,
    w_mod,
    norm_gain,
    w_query,
    w_key,
    w_value,
    w_outgate,
    w_decay,
    w_beta,
    decay_rate,
    decay_bias,
    extra_decay,
    out_gain,
    w_out,
):
    operands = {
        "cond": cond,
        "ctx_cond": ctx_cond[None, :],
        "w_mod": w_mod,
        "latent": latent,
        "context": context,
        "gain": norm_gain.reshape(D // HEAD, HEAD),
        "w_key": w_key,
        "w_value": w_value,
        "w_decay": jnp.transpose(w_decay, (1, 2, 0)),
        "w_beta": jnp.transpose(w_beta, (1, 2, 0)),
        "extra": extra_decay,
        "w_query": w_query,
        "w_outgate": w_outgate,
        "out_gain": out_gain[None, :],
        "w_out": w_out,
        "rate": decay_rate,
        "bias": decay_bias,
    }
    sizes = [lax.axis_size(name) for name in (ZAX, XAX, YAX)]
    return whole(operands, *sizes)[None]


def solution(mesh):
    torus = Mesh(
        mesh.devices.reshape(-1, 4, mesh.shape["tp"], mesh.shape["dp"]), (ZAX, XAX, YAX, "dp")
    )
    return jax.shard_map(
        on_device,
        mesh=torus,
        in_specs=(
            P("dp", SP, None),
            P("dp", SP),
            P("dp", SP, None),
            P(SP),
            P(SP, "tp"),
            P(),
            P(None, "tp"),
            P(None, "tp"),
            P(None, "tp"),
            P(None, "tp"),
            P(None, None, "tp"),
            P(None, None, "tp"),
            P(None, "tp"),
            P(None, "tp"),
            P("dp", None, "tp", SP),
            P(),
            P(),
        ),
        out_specs=P("dp", SP_TP, None),
        check_vma=False,
    )
```
